256 devices in a mesh: ep: 64 (over z, x, core), tp: 4 (over y).
Axes of the slice: x: 4, y: 4, z: 8, core: 2. Of those that a mesh axis runs over, the one named last changes fastest.
Arguments:
- tokens: bfloat16 [16384, 2048], P('ep'), may hold values from -6 to 6
- routes: int32 [16384, 4], P('ep'), may hold values from 0 to 63, all different within a row; in each aligned block of 256 rows (0 to 255, 256 to 511, ...) at most 20 rows name the same one
- gate_weights: float32 [16384, 4], P('ep'), may hold values from 0.05 to 1
- out_grad: bfloat16 [16384, 2048], P('ep'), may hold values from -0.59765625 to 0.59765625
- w_gate: bfloat16 [64, 2048, 1024], P('ep', None, 'tp'), may hold values from -0.1875 to 0.1875
- w_up: bfloat16 [64, 2048, 1024], P('ep', None, 'tp'), may hold values from -0.1875 to 0.1875
- w_down: bfloat16 [64, 1024, 2048], P('ep', 'tp'), may hold values from -0.1875 to 0.1875
Outputs:
- token_grad: bfloat16 [16384, 2048], P('ep', 'tp')
- gate_grad: float32 [16384, 4], P('ep')
- gate_weight_grad: float32 [64, 2048, 1024], P('ep', None, 'tp')
- up_weight_grad: float32 [64, 2048, 1024], P('ep', None, 'tp')
- down_weight_grad: float32 [64, 1024, 2048], P('ep', 'tp')
The draws below stay inside these ranges and needn't reach their ends.
Inputs may be any that keep to these rules, and one draw needn't show every extreme that they name: `routes`: each row names 4 different experts. In each aligned block of 256 rows (the rows of one device) no expert is named by more than 20 rows, and in some block an expert is named by exactly 20 rows.
All inputs are finite; a program needn't handle non-finite values.
Results may differ from the reference program's by a relative error of at most 0.012.
Values may be sent and summed in bfloat16 or wider, within the bound.
No kernel may reach another device: no remote copies, remote signals or barrier semaphores. Data moves between devices by JAX's collectives and lax.ppermute only.
A program may use at most 128 MiB of HBM per device.

```python
import math
import jax
import jax.numpy as jnp
import numpy as np
from jax import lax

D = 2048
FF = 1024
TOPK = 4
TOK_DEV = 256
EXPERTS = 64
TOKENS = 16384
CAP = 20
N_EP = 64
N_TP = 4


def steps_of(rng, extent, split, smallest, high):
    def one(axis_at, parts):
        heights = jax.random.uniform(jax.random.fold_in(jax.random.fold_in(rng, 6), axis_at), (parts,), jnp.float32, smallest / len(split), high / len(split))
        return jnp.repeat(jnp.exp(heights), extent[axis_at] // parts).reshape((-1,) + (1,) * (len(extent) - axis_at - 1))

    gain = one(*split[0])
    for cut in split[1:]:
        gain = gain * one(*cut)
    return gain


def assign_block(key, own, number, rows, amount, top, reach, lean):
    ranking = jax.random.permutation(key, amount)
    crowded, usual = portions_of(amount, rows * top, reach, lean, True), portions_of(amount, rows * top, reach, lean, False)
    places = jnp.arange(amount)

    def named(sizes, rotation):
        used = int((sizes > 0).sum())
        fixed = max(1, used // 4)
        moved = fixed + (places - fixed + rotation * (used - fixed)) % max(1, amount - fixed)
        return jnp.zeros((amount,), jnp.int32).at[ranking[jnp.where(places < fixed, places, moved)]].set(jnp.asarray(sizes, jnp.int32))

    sizes = jnp.where(number % 4 == 0, named(crowded, number // 4), named(usual, number - number // 4 - 1))
    mixed = jax.random.permutation(jax.random.fold_in(own, 3), amount)
    source_of, receiver = mixed[0:amount // 2 * 2:2], mixed[1:amount // 2 * 2:2]
    margin = jnp.minimum(sizes[source_of] - 1, reach - sizes[receiver]) // 2
    margin = jnp.where((source_of == ranking[0]) | (receiver == ranking[0]) | (sizes[receiver] == 0), 0, jnp.maximum(margin, 0))
    moved = jax.random.randint(jax.random.fold_in(own, 4), (amount // 2,), 0, 1 << 20) % (margin + 1)
    sizes = sizes.at[source_of].add(-moved).at[receiver].add(moved)
    labels = jnp.searchsorted(jnp.cumsum(sizes), jnp.arange(rows * top), side="right").astype(jnp.int32)
    grid = labels.reshape(top, rows).T
    grid = grid[jax.random.permutation(jax.random.fold_in(own, 1), rows)]
    rotation = jax.random.randint(jax.random.fold_in(own, 2), (rows, 1), 0, top)
    return jnp.take_along_axis(grid, (jnp.arange(top)[None, :] + rotation) % top, axis=1)


def portions_of(count, total, reach, lean, full):
    weights = [(1 << 20) // math.isqrt(rank ** lean) + 1 for rank in range(1, count + 1)]
    largest = reach if full else min(reach, max(-(-total // count), total * weights[0] // sum(weights)))
    least = 1 if total - largest >= count - 1 else 0
    given, surplus = [largest] + [least] * (count - 1), total - largest - least * (count - 1)
    while surplus > 0:
        movable = [i for i in range(1, count) if given[i] < largest] or [i for i in range(1, count) if given[i] < reach]
        mass, remaining = sum([weights[i] for i in movable]), surplus
        for i in movable:
            more = min(reach - given[i], max(1, remaining * weights[i] // mass), surplus)
            given[i] = given[i] + more
            surplus = surplus - more
    return np.array(given)


def bell_draw(key, extent, scale, bound, shards=(), kind=jnp.bfloat16):
    values = jax.random.normal(key, extent, jnp.float32) * scale
    if len(shards) > 0:
        values = steps_of(key, extent, shards, -0.22, 0.18) * values
    return jnp.clip(values, min=-bound, max=bound).astype(kind)


def setup_inputs(seed: int = 0) -> dict:
    key_of = jax.random.split(jax.random.key(seed), 8)
    tokens = bell_draw(key_of[0], (TOKENS, D), 1.0, 6.0, ((0, 64),))
    routes_keys = jax.random.split(jax.random.fold_in(key_of[1], 1), TOKENS // TOK_DEV)
    routes_turns = jax.random.permutation(jax.random.fold_in(key_of[1], 3), TOKENS // TOK_DEV)
    routes = jax.vmap(lambda own, number: assign_block(jax.random.fold_in(key_of[1], 2), own, number, TOK_DEV, EXPERTS, TOPK, CAP, 1))(routes_keys, routes_turns).reshape((TOKENS, TOPK))
    gate_weights = jnp.clip(jnp.exp(math.log(1.0) - 2.9957323 * jax.random.uniform(key_of[2], (TOKENS, TOPK), jnp.float32) ** steps_of(key_of[2], (TOKENS, TOPK), ((0, 64),), -0.2, 0.2)), 0.05, 1.0)
    out_grad = bell_draw(key_of[3], (TOKENS, D), 0.1, 0.59765625, ((0, 64),))
    w_gate = bell_draw(key_of[4], (EXPERTS, D, FF), (D // 2) ** -0.5, 0.1875, ((0, 64), (2, 4)))
    w_up = bell_draw(key_of[5], (EXPERTS, D, FF), (D // 2) ** -0.5, 0.1875, ((0, 64), (2, 4)))
    w_down = bell_draw(key_of[6], (EXPERTS, FF, D), FF ** -0.5, 0.1875, ((0, 64), (1, 4)))
    return dict(tokens=tokens, routes=routes, gate_weights=gate_weights, out_grad=out_grad, w_gate=w_gate, w_up=w_up, w_down=w_down)


clamp_limit = 7.0
sigmoid_slope = 1.702


def unit_backward(gate_pre, up_pre, hidden_grad):
    glu = jnp.minimum(gate_pre, clamp_limit)
    linear = jnp.clip(up_pre, -clamp_limit, clamp_limit)
    sigma = jax.nn.sigmoid(sigmoid_slope * glu)
    active = glu * sigma
    hidden = (active * (linear + 1.0)).astype(jnp.bfloat16)
    slope_term = sigma + sigmoid_slope * active * (1.0 - sigma)
    gate_pre_grad = jnp.where(gate_pre < clamp_limit, hidden_grad * (linear + 1.0) * slope_term, 0.0).astype(jnp.bfloat16)
    up_pre_grad = jnp.where(jnp.abs(up_pre) < clamp_limit, hidden_grad * active, 0.0).astype(jnp.bfloat16)
    return hidden, gate_pre_grad, up_pre_grad


def block_round_total(partial_value):
    rounded = lax.optimization_barrier(partial_value.astype(jnp.bfloat16))
    return jnp.sum(rounded.astype(jnp.float32), axis=0)


def reference(tokens, routes, gate_weights, out_grad, w_gate, w_up, w_down):
    blocks = routes.reshape(N_EP, TOK_DEV * TOPK)
    onehot = (blocks[:, :, None] == jnp.arange(EXPERTS, dtype=jnp.int32)[None, None, :]).astype(jnp.int32)
    slot_rank = jnp.sum((jnp.cumsum(onehot, axis=1) - onehot) * onehot, axis=2)
    source = jnp.arange(N_EP, dtype=jnp.int32)[:, None]
    target = (blocks * (N_EP * CAP) + source * CAP + slot_rank).reshape(-1)
    pair_index = jnp.arange(TOKENS * TOPK, dtype=jnp.int32)
    pair_table = jnp.zeros((EXPERTS * N_EP * CAP,), jnp.int32).at[target].set(pair_index)
    filled = jnp.zeros((EXPERTS * N_EP * CAP,), jnp.int32).at[target].set(1)
    flat_weights = gate_weights.reshape(-1)
    row_count = N_EP * CAP

    def per_expert(running, expert):
        token_acc, gate_acc = running
        slot_pairs = lax.dynamic_slice_in_dim(pair_table, expert * row_count, row_count)
        is_live = lax.dynamic_slice_in_dim(filled, expert * row_count, row_count)[:, None] > 0
        token_index = slot_pairs // TOPK
        x_rows = jnp.where(is_live, tokens[token_index], jnp.zeros((), jnp.bfloat16))
        dy_rows = out_grad[token_index]
        scaled = jnp.where(is_live, flat_weights[slot_pairs][:, None] * dy_rows.astype(jnp.float32), 0.0).astype(jnp.bfloat16)
        gate_mat = w_gate[expert]
        up_mat = w_up[expert]
        down_mat = w_down[expert]
        gate_pre = jnp.dot(x_rows, gate_mat, preferred_element_type=jnp.float32)
        up_pre = jnp.dot(x_rows, up_mat, preferred_element_type=jnp.float32)
        hidden_grad = jnp.dot(scaled, down_mat.T, preferred_element_type=jnp.float32)
        hidden, gate_pre_grad, up_pre_grad = unit_backward(gate_pre, up_pre, hidden_grad)
        unit_block = FF // N_TP
        gate_blocks = gate_pre_grad.astype(jnp.float32).reshape(row_count, N_TP, unit_block)
        up_blocks = up_pre_grad.astype(jnp.float32).reshape(row_count, N_TP, unit_block)
        hidden_blocks = hidden.astype(jnp.float32).reshape(row_count, N_TP, unit_block)
        gate_mat_blocks = gate_mat.astype(jnp.float32).reshape(D, N_TP, unit_block)
        up_mat_blocks = up_mat.astype(jnp.float32).reshape(D, N_TP, unit_block)
        down_blocks = down_mat.astype(jnp.float32).reshape(N_TP, unit_block, D)
        row_partial = jnp.einsum('rnf,dnf->nrd', gate_blocks, gate_mat_blocks) + jnp.einsum('rnf,dnf->nrd', up_blocks, up_mat_blocks)
        row_grad = block_round_total(row_partial).astype(jnp.bfloat16)
        expert_out = block_round_total(jnp.einsum('rnf,nfd->nrd', hidden_blocks, down_blocks))
        token_acc = token_acc.at[token_index].add(jnp.where(is_live, row_grad.astype(jnp.float32), 0.0))
        products = jnp.sum(dy_rows.astype(jnp.float32) * expert_out, axis=1)
        gate_acc = gate_acc.at[slot_pairs].add(jnp.where(is_live[:, 0], products, 0.0))
        gate_weight_grad = jnp.dot(x_rows.T, gate_pre_grad, preferred_element_type=jnp.float32)
        up_weight_grad = jnp.dot(x_rows.T, up_pre_grad, preferred_element_type=jnp.float32)
        down_weight_grad = jnp.dot(hidden.T, scaled, preferred_element_type=jnp.float32)
        return (token_acc, gate_acc), (gate_weight_grad, up_weight_grad, down_weight_grad)

    start = (jnp.zeros((TOKENS, D), jnp.float32), jnp.zeros((TOKENS * TOPK,), jnp.float32))
    (token_acc, gate_acc), grads = lax.scan(per_expert, start, jnp.arange(EXPERTS, dtype=jnp.int32))
    return (token_acc.astype(jnp.bfloat16), gate_acc.reshape(TOKENS, TOPK), grads[0], grads[1], grads[2])
```

```python
import jax
import jax.numpy as jnp
from jax import lax
from jax.sharding import Mesh
from jax.sharding import PartitionSpec as P


EP = ("ep_0", "ep_1", "ep_2")
ZX = ("ep_0", "ep_1")
CY = ("ep_2", "tp")

clamp_limit = 7.0
sigmoid_slope = 1.702
bf16 = jnp.bfloat16
f32 = jnp.float32

SWAP = [(4, 3), (3, 4), (5, 2), (2, 5)]
PAIR_AWAY = [(4, 5), (5, 4), (2, 3), (3, 2)]
PAIR_HOME = [(0, 1), (1, 0), (6, 7), (7, 6)]
CORES = [(0, 1), (1, 0)]


def dot(a, b, dims, out=f32):
    return lax.dot_general(a, b, (dims, ((), ())), preferred_element_type=out)


def unit_backward(gate_pre, up_pre, hidden_grad):
    glu = jnp.minimum(gate_pre, clamp_limit)
    linear = jnp.clip(up_pre, -clamp_limit, clamp_limit)
    sigma = jax.nn.sigmoid(sigmoid_slope * glu)
    active = glu * sigma
    hidden = (active * (linear + 1.0)).astype(bf16)
    slope_term = sigma + sigmoid_slope * active * (1.0 - sigma)
    gate_pre_grad = jnp.where(
        gate_pre < clamp_limit, hidden_grad * (linear + 1.0) * slope_term, 0.0
    ).astype(bf16)
    up_pre_grad = jnp.where(jnp.abs(up_pre) < clamp_limit, hidden_grad * active, 0.0).astype(bf16)
    return hidden, gate_pre_grad, up_pre_grad


def in_parts(v):
    hi = lax.reduce_precision(v, 8, 7)
    mid = lax.reduce_precision(v - hi, 8, 7)
    low = lax.reduce_precision(v - hi - mid, 8, 7)
    return hi.astype(bf16), mid.astype(bf16), low.astype(bf16)


def quarters_to_rows(tail):
    w = tail.shape[1]
    return tail.reshape(32, 4, 2, w).transpose(0, 2, 1, 3).reshape(64, 4 * w)


def rows_to_quarters(rows):
    w = rows.shape[1] // 4
    return rows.reshape(32, 2, 4, w).transpose(0, 2, 1, 3).reshape(256, w)


def layer(tokens, routes, gate_weights, out_grad, w_gate, w_up, w_down):
    y = lax.axis_index("tp")
    core = lax.axis_index("ep_2")
    kind = y // 2
    part = y % 2
    stays = core == kind

    home = (w_gate[0], w_up[0], w_down[0])
    swapped = [lax.ppermute(w, CY, SWAP) for w in home]
    paired = [lax.ppermute(w, CY, PAIR_HOME) for w in home]
    paired_away = [lax.ppermute(w, CY, PAIR_AWAY) for w in swapped]
    first = lax.optimization_barrier([jnp.where(stays, a, b) for a, b in zip(home, swapped)])
    second = lax.optimization_barrier([jnp.where(stays, a, b) for a, b in zip(paired, paired_away)])

    routes_t = routes.T
    weights_t = gate_weights.T
    expert = 2 * jnp.arange(32, dtype=jnp.int32)[:, None] + kind
    hit = [routes_t[k][None, :] == expert for k in range(4)]
    named = hit[0] | hit[1] | hit[2] | hit[3]
    named_bf = named.astype(bf16)
    before = (jnp.arange(256)[:, None] < jnp.arange(256)[None, :]).astype(bf16)
    rank = dot(named_bf, before, ((1,), (0,))).astype(jnp.int32) - 10 * part
    key = jnp.where(named & (rank >= 0) & (rank < 10), rank, -1)
    weight_of = sum(jnp.where(hit[k], weights_t[k][None, :], 0.0) for k in range(4))
    eight = jnp.arange(8, dtype=jnp.int32)[None, :, None]
    in_main = (key[:, None, :] == eight).reshape(256, 256)
    in_tail = (key[:, None, :] == 8 + eight % 2).reshape(256, 256)
    slot_weight = jnp.broadcast_to(weight_of[:, None, :], (32, 8, 256)).reshape(256, 256)
    blocks = []
    quarter = ((jnp.arange(256) % 8) // 2)[:, None]
    for src in (tokens, out_grad):
        for sel in (in_main, in_tail):
            got = dot(sel.astype(bf16), src, ((1,), (0,)))
            if src is out_grad:
                got = got * jnp.sum(jnp.where(sel, slot_weight, 0.0), axis=1, keepdims=True)
            if sel is in_tail:
                got = sum(
                    jnp.where(quarter == q, got[:, 512 * q : 512 * q + 512], 0.0) for q in range(4)
                )
            blocks.append(got.astype(bf16))
    x_main, x_tail, g_main, g_tail = blocks
    send = jnp.concatenate([x_main, g_main, x_tail, g_tail], axis=1).reshape(32, 8, 5120)
    mine = lax.all_to_all(send, ZX, 0, 0, tiled=True)
    other = lax.ppermute(mine, "ep_2", CORES)
    xs, gs = [], []
    for got in (mine.reshape(256, 5120), other.reshape(256, 5120)):
        xs += [got[:, :2048], quarters_to_rows(got[:, 4096:4608])]
        gs += [got[:, 2048:4096], quarters_to_rows(got[:, 4608:])]
    x = jnp.concatenate(xs, axis=0)
    g = jnp.concatenate(gs, axis=0)

    row_part = 0.0
    product = 0.0
    acts = []
    for wg, wu, wd in (first, second):
        gate_pre = dot(x, wg, ((1,), (0,)))
        up_pre = dot(x, wu, ((1,), (0,)))
        hidden_grad = dot(g, wd, ((1,), (1,)))
        hidden, gg, ug = unit_backward(gate_pre, up_pre, hidden_grad)
        acts.append((hidden, gg, ug))
        product = product + jnp.sum(hidden.astype(f32) * hidden_grad, axis=1)
        row_part = row_part + dot(gg, wg, ((1,), (1,))) + dot(ug, wu, ((1,), (1,)))

    def weight_grads(h, gg, ug):
        return (
            dot(x, gg, ((0,), (0,))),
            dot(x, ug, ((0,), (0,))),
            dot(h, g, ((0,), (0,))),
        )

    away = [w.astype(bf16) for w in weight_grads(*acts[1])]
    kept = weight_grads(*acts[0])
    got_away = [lax.ppermute(w, CY, PAIR_AWAY) for w in away]
    tied = lax.optimization_barrier((tuple(away), tuple(got_away)))
    away, got_away = tied
    got_home = [lax.ppermute(w, CY, PAIR_HOME) for w in away]
    moved = [
        lax.ppermute((a + b.astype(f32)).astype(bf16), CY, SWAP) for a, b in zip(kept, got_away)
    ]
    grads = [
        jnp.where(stays, a + b.astype(f32), m.astype(f32))[None]
        for a, b, m in zip(kept, got_home, moved)
    ]

    hand_over = jnp.concatenate(
        [row_part[320:].astype(bf16)]
        + [jnp.pad(v[:, None], ((0, 0), (0, 0))) for v in in_parts(product[320:])]
        + [jnp.zeros((320, 125), bf16)],
        axis=1,
    )
    handed = lax.ppermute(hand_over, "ep_2", CORES).astype(f32)
    row_grad = (row_part[:320] + handed[:, :2048]).astype(bf16)
    product = product[:320] + handed[:, 2048] + handed[:, 2049] + handed[:, 2050]
    main_parts = jnp.stack(in_parts(product[:256]), axis=1)
    tail_product = jnp.broadcast_to(product[256:].reshape(32, 1, 2), (32, 4, 2)).reshape(256)
    tail_parts = jnp.stack(in_parts(tail_product), axis=1)
    back = jnp.concatenate(
        [
            row_grad[:256],
            rows_to_quarters(row_grad[256:]),
            main_parts,
            tail_parts,
            jnp.zeros((256, 122), bf16),
        ],
        axis=1,
    ).reshape(32, 8, 2688)
    back = lax.all_to_all(back, ZX, 0, 0, tiled=True).reshape(256, 2688)
    tail_rows = quarters_to_rows(back[:, 2048:2560])
    in_tail_rows = in_tail.reshape(32, 8, 256)[:, :2].reshape(64, 256)
    token_part = dot(in_main.astype(bf16), back[:, :2048], ((0,), (0,))) + dot(
        in_tail_rows.astype(bf16), tail_rows, ((0,), (0,))
    )
    parts = back[:, 2560:2566].astype(f32)
    main_product = (parts[:, 0] + parts[:, 1] + parts[:, 2])[:, None]
    tail_product = (parts[:, 3] + parts[:, 4] + parts[:, 5]).reshape(32, 8)[:, :2].reshape(64, 1)
    of_token = jnp.sum(
        jnp.where(in_main, main_product, 0.0).reshape(32, 8, 256), axis=1
    ) + jnp.sum(jnp.where(in_tail_rows, tail_product, 0.0).reshape(32, 2, 256), axis=1)
    pair_product = jnp.stack(
        [jnp.sum(jnp.where(hit[k], of_token, 0.0), axis=0) for k in range(4)], axis=0
    )

    def block_for(dest):
        cols = lax.dynamic_slice_in_dim(token_part, 512 * dest, 512, 1)
        return cols

    token_sum = block_for(y)
    own_parts = in_parts(pair_product)
    product_sum = sum(v.astype(f32) for v in own_parts)
    flat = jnp.concatenate(own_parts + (jnp.zeros((4, 256), bf16),), axis=0)
    flat = jnp.concatenate([flat, jnp.zeros((16, 256), bf16)], axis=1)
    for shift in (1, 2, 3):
        dest = (y + shift) % 4
        message = jnp.concatenate([block_for(dest).astype(bf16), flat], axis=0)
        got = lax.ppermute(message, "tp", [(i, (i + shift) % 4) for i in range(4)]).astype(f32)
        token_sum = token_sum + got[:256]
        product_sum = product_sum + got[256:260, :256] + got[260:264, :256] + got[264:268, :256]
    token_grad = token_sum.astype(bf16)
    gate_grad = (product_sum / weights_t).T
    return (token_grad, gate_grad, grads[0], grads[1], grads[2])


def solution(mesh):
    finer = Mesh(mesh.devices.reshape(8, 4, 2, mesh.shape["tp"]), ("ep_0", "ep_1", "ep_2", "tp"))
    in_specs = (
        P(EP, None),
        P(EP, None),
        P(EP, None),
        P(EP, None),
        P(EP, None, "tp"),
        P(EP, None, "tp"),
        P(EP, "tp", None),
    )
    out_specs = (P(EP, "tp"), P(EP, None), P(EP, None, "tp"), P(EP, None, "tp"), P(EP, "tp", None))
    return jax.shard_map(layer, mesh=finer, in_specs=in_specs, out_specs=out_specs, check_vma=False)
```

```python
import jax
import jax.numpy as jnp
from jax import lax
from jax.experimental import pallas as pl
from jax.experimental.pallas import tpu as pltpu
from jax.sharding import Mesh
from jax.sharding import PartitionSpec as P


EP = ("ep_0", "ep_1", "ep_2")
ZX = ("ep_0", "ep_1")
CY = ("ep_2", "tp")

clamp_limit = 7.0
sigmoid_slope = 1.702
bf16 = jnp.bfloat16
f32 = jnp.float32

SWAP = [(4, 3), (3, 4), (5, 2), (2, 5)]
PAIR_AWAY = [(4, 5), (5, 4), (2, 3), (3, 2)]
PAIR_HOME = [(0, 1), (1, 0), (6, 7), (7, 6)]
CORES = [(0, 1), (1, 0)]


def dot(a, b, dims, out=f32):
    return lax.dot_general(a, b, (dims, ((), ())), preferred_element_type=out)


def unit_backward(gate_pre, up_pre, hidden_grad):
    glu = jnp.minimum(gate_pre, clamp_limit)
    linear = jnp.clip(up_pre, -clamp_limit, clamp_limit)
    sigma = jax.nn.sigmoid(sigmoid_slope * glu)
    active = glu * sigma
    hidden = (active * (linear + 1.0)).astype(bf16)
    slope_term = sigma + sigmoid_slope * active * (1.0 - sigma)
    gate_pre_grad = jnp.where(
        gate_pre < clamp_limit, hidden_grad * (linear + 1.0) * slope_term, 0.0
    ).astype(bf16)
    up_pre_grad = jnp.where(jnp.abs(up_pre) < clamp_limit, hidden_grad * active, 0.0).astype(bf16)
    return hidden, gate_pre_grad, up_pre_grad


def in_parts(v):
    hi = lax.reduce_precision(v, 8, 7)
    mid = lax.reduce_precision(v - hi, 8, 7)
    low = lax.reduce_precision(v - hi - mid, 8, 7)
    return hi.astype(bf16), mid.astype(bf16), low.astype(bf16)


def call(body, out_shape, *operands, scratch=()):
    vmem = pl.BlockSpec(memory_space=pltpu.VMEM)
    return pl.pallas_call(
        body,
        out_shape=out_shape,
        in_specs=[vmem] * len(operands),
        out_specs=[vmem] * len(out_shape) if isinstance(out_shape, (list, tuple)) else vmem,
        compiler_params=pltpu.CompilerParams(vmem_limit_bytes=60 * 2**20),
    )(*operands)


def tail_pick(quarter):
    row = lax.broadcasted_iota(jnp.int32, (64, 256), 0)
    col = lax.broadcasted_iota(jnp.int32, (64, 256), 1)
    return (col == (row // 2) * 8 + quarter * 2 + row % 2).astype(f32).astype(bf16)


def tail_place(quarter):
    row = lax.broadcasted_iota(jnp.int32, (256, 64), 1)
    col = lax.broadcasted_iota(jnp.int32, (256, 64), 0)
    return (col == (row // 2) * 8 + quarter * 2 + row % 2).astype(f32).astype(bf16)


def expand(src, x, g, at):
    x[at : at + 256, :] = src[:, :2048]
    g[at : at + 256, :] = src[:, 2048:4096]
    for q in range(4):
        cols = slice(512 * q, 512 * q + 512)
        pick = tail_pick(q)
        x[at + 256 : at + 320, cols] = dot(pick, src[:, 4096:4608], ((1,), (0,))).astype(bf16)
        g[at + 256 : at + 320, cols] = dot(pick, src[:, 4608:5120], ((1,), (0,))).astype(bf16)


def units(x, g, acts, product, at, weights):
    rows = slice(at, at + 320)
    total = jnp.zeros((320, 1), f32)
    for s, (wg, wu, wd) in enumerate(weights):
        gate_pre = dot(x[rows, :], wg[...], ((1,), (0,)))
        up_pre = dot(x[rows, :], wu[...], ((1,), (0,)))
        hidden_grad = dot(g[rows, :], wd[...], ((1,), (1,)))
        hidden, gg, ug = unit_backward(gate_pre, up_pre, hidden_grad)
        to = 768 * s
        acts[rows, to : to + 256] = hidden
        acts[rows, to + 256 : to + 512] = gg
        acts[rows, to + 512 : to + 768] = ug
        total = total + jnp.sum(hidden.astype(f32) * hidden_grad, axis=1, keepdims=True)
    product[...] = jnp.broadcast_to(total, (320, 128))


def act_mine_body(mine, wg1, wu1, wd1, wg2, wu2, wd2, x, g, acts, product):
    expand(mine, x, g, 0)
    units(x, g, acts, product, 0, ((wg1, wu1, wd1), (wg2, wu2, wd2)))


def act_other_body(
    other, xm, gm, actm, wg1, wu1, wd1, wg2, wu2, wd2, x, g, acts, product, ag, au, ad
):
    x[:320, :] = xm[...]
    g[:320, :] = gm[...]
    acts[:320, :] = actm[...]
    expand(other, x, g, 320)
    units(x, g, acts, product, 320, ((wg1, wu1, wd1), (wg2, wu2, wd2)))

    def chunk(d, carry):
        cols = pl.ds(pl.multiple_of(d * 256, 256), 256)
        both = dot(x[:, cols], acts[:, 1024:1536], ((0,), (0,)))
        ag[cols, :] = both[:, :256].astype(bf16)
        au[cols, :] = both[:, 256:].astype(bf16)
        return carry

    lax.fori_loop(0, 8, chunk, 0)
    ad[...] = dot(acts[:, 768:1024], g[...], ((0,), (0,))).astype(bf16)


def act_mine_call(*operands):
    shape = jax.ShapeDtypeStruct
    outs = [
        shape((320, 2048), bf16),
        shape((320, 2048), bf16),
        shape((320, 1536), bf16),
        shape((320, 128), f32),
    ]
    return call(act_mine_body, outs, *operands)


def act_other_call(*operands):
    shape = jax.ShapeDtypeStruct
    outs = [
        shape((640, 2048), bf16),
        shape((640, 2048), bf16),
        shape((640, 1536), bf16),
        shape((320, 128), f32),
        shape((2048, 256), bf16),
        shape((2048, 256), bf16),
        shape((256, 2048), bf16),
    ]
    return call(act_other_body, outs, *operands)


def kernel_parts(v):
    hi = v.astype(bf16)
    mid = (v - hi.astype(f32)).astype(bf16)
    low = (v - hi.astype(f32) - mid.astype(f32)).astype(bf16)
    return hi, mid, low


def row_sum(acts, rows, cols, weights):
    wg1, wu1, wg2, wu2 = weights
    total = jnp.zeros((320, 256), f32)
    for to, w in ((256, wg1), (512, wu1), (1024, wg2), (1280, wu2)):
        total = total + dot(acts[rows, to : to + 256], w[cols, :], ((1,), (1,)))
    return total


def row_other_body(acts, product, wg1, wu1, wg2, wu2, hand_over):
    def chunk(d, carry):
        cols = pl.ds(pl.multiple_of(d * 256, 256), 256)
        total = row_sum(acts, slice(320, 640), cols, (wg1, wu1, wg2, wu2))
        hand_over[:, cols] = total.astype(bf16)
        return carry

    lax.fori_loop(0, 8, chunk, 0)
    hi, mid, low = kernel_parts(product[...])
    lane = lax.broadcasted_iota(jnp.int32, (320, 128), 1)
    hand_over[:, 2048:] = jnp.where(
        lane == 0, hi.astype(f32), jnp.where(lane == 1, mid.astype(f32), low.astype(f32))
    ).astype(bf16)


def row_mine_body(acts, wg1, wu1, wg2, wu2, own):
    def chunk(d, carry):
        cols = pl.ds(pl.multiple_of(d * 256, 256), 256)
        own[:, cols] = row_sum(acts, slice(0, 320), cols, (wg1, wu1, wg2, wu2))
        return carry

    lax.fori_loop(0, 8, chunk, 0)


def row_other_call(*operands):
    return call(row_other_body, jax.ShapeDtypeStruct((320, 2176), bf16), *operands)


def row_mine_call(*operands):
    return call(row_mine_body, jax.ShapeDtypeStruct((320, 2048), f32), *operands)


def back_body(own, product, handed, back):
    back[:, :2048] = (own[:256, :] + handed[:256, :2048].astype(f32)).astype(bf16)
    tail = (own[256:320, :] + handed[256:320, :2048].astype(f32)).astype(bf16)
    lane = lax.broadcasted_iota(jnp.int32, (320, 128), 1)
    got = jnp.sum(
        jnp.where(lane < 3, handed[:, 2048:].astype(f32), 0.0), axis=1, keepdims=True
    )
    total = product[...] + got
    hi, mid, low = kernel_parts(total)
    spread = jnp.where(
        lane == 0, hi.astype(f32), jnp.where(lane == 1, mid.astype(f32), low.astype(f32))
    )
    placed = jnp.zeros((256, 512), f32)
    weights = jnp.zeros((256, 128), f32)
    for q in range(4):
        place = tail_place(q)
        placed = placed + dot(place, tail[:, 512 * q : 512 * q + 512], ((1,), (0,)))
        weights = weights + dot(place, spread[256:320].astype(bf16), ((1,), (0,)))
    back[:, 2048:2560] = placed.astype(bf16)
    back[:, 2560:2688] = jnp.where(lane[:256] < 3, spread[:256], 0.0).astype(bf16) + jnp.where(
        (lane[:256] >= 3) & (lane[:256] < 6), pltpu.roll(weights, 3, 1), 0.0
    ).astype(bf16)


def back_call(*operands):
    return call(back_body, jax.ShapeDtypeStruct((256, 2688), bf16), *operands)


def quarters_to_rows(tail):
    w = tail.shape[1]
    return tail.reshape(32, 4, 2, w).transpose(0, 2, 1, 3).reshape(64, 4 * w)


def layer(tokens, routes, gate_weights, out_grad, w_gate, w_up, w_down):
    y = lax.axis_index("tp")
    core = lax.axis_index("ep_2")
    kind = y // 2
    part = y % 2
    stays = core == kind

    home = (w_gate[0], w_up[0], w_down[0])
    swapped = [lax.ppermute(w, CY, SWAP) for w in home]
    paired = [lax.ppermute(w, CY, PAIR_HOME) for w in home]
    paired_away = [lax.ppermute(w, CY, PAIR_AWAY) for w in swapped]
    first = lax.optimization_barrier([jnp.where(stays, a, b) for a, b in zip(home, swapped)])
    second = lax.optimization_barrier([jnp.where(stays, a, b) for a, b in zip(paired, paired_away)])

    routes_t = routes.T
    weights_t = gate_weights.T
    expert = 2 * jnp.arange(32, dtype=jnp.int32)[:, None] + kind
    hit = [routes_t[k][None, :] == expert for k in range(4)]
    named = hit[0] | hit[1] | hit[2] | hit[3]
    named_bf = named.astype(bf16)
    before = (jnp.arange(256)[:, None] < jnp.arange(256)[None, :]).astype(bf16)
    rank = dot(named_bf, before, ((1,), (0,))).astype(jnp.int32) - 10 * part
    key = jnp.where(named & (rank >= 0) & (rank < 10), rank, -1)
    weight_of = sum(jnp.where(hit[k], weights_t[k][None, :], 0.0) for k in range(4))
    eight = jnp.arange(8, dtype=jnp.int32)[None, :, None]
    in_main = (key[:, None, :] == eight).reshape(256, 256)
    in_tail = (key[:, None, :] == 8 + eight % 2).reshape(256, 256)
    slot_weight = jnp.broadcast_to(weight_of[:, None, :], (32, 8, 256)).reshape(256, 256)
    blocks = []
    quarter = ((jnp.arange(256) % 8) // 2)[:, None]
    for src in (tokens, out_grad):
        for sel in (in_main, in_tail):
            got = dot(sel.astype(bf16), src, ((1,), (0,)))
            if src is out_grad:
                got = got * jnp.sum(jnp.where(sel, slot_weight, 0.0), axis=1, keepdims=True)
            if sel is in_tail:
                got = sum(
                    jnp.where(quarter == q, got[:, 512 * q : 512 * q + 512], 0.0) for q in range(4)
                )
            blocks.append(got.astype(bf16))
    x_main, x_tail, g_main, g_tail = blocks
    send = jnp.concatenate([x_main, g_main, x_tail, g_tail], axis=1).reshape(32, 8, 5120)
    mine = lax.all_to_all(send, ZX, 0, 0, tiled=True)
    other = lax.ppermute(mine, "ep_2", CORES)
    xm, gm, actm, product = act_mine_call(mine.reshape(256, 5120), *first, *second)
    x, g, acts, product_other, *away = act_other_call(
        other.reshape(256, 5120), xm, gm, actm, *first, *second
    )
    hidden, gg, ug = acts[:, :256], acts[:, 256:512], acts[:, 512:768]
    kept = (
        dot(x, gg, ((0,), (0,))),
        dot(x, ug, ((0,), (0,))),
        dot(hidden, g, ((0,), (0,))),
    )
    kept = lax.optimization_barrier(kept)
    got_away, moved = [], []
    for i in range(3):
        got_away.append(lax.ppermute(away[i], CY, PAIR_AWAY))
        total = (kept[i] + got_away[i].astype(f32)).astype(bf16)
        moved.append(lax.ppermute(total, CY, SWAP))
    tied = lax.optimization_barrier((*away, *got_away))[:3]
    got_home = [lax.ppermute(w, CY, PAIR_HOME) for w in tied]
    grads = [
        jnp.where(stays, a + b.astype(f32), m.astype(f32))[None]
        for a, b, m in zip(kept, got_home, moved)
    ]

    row_weights = (first[0], first[1], second[0], second[1])
    hand_over = row_other_call(acts, product_other, *row_weights)
    handed = lax.ppermute(hand_over, "ep_2", CORES)
    own_part = row_mine_call(actm, *row_weights)
    back = back_call(own_part, product, handed).reshape(32, 8, 2688)
    back = lax.all_to_all(back, ZX, 0, 0, tiled=True).reshape(256, 2688)
    tail_rows = quarters_to_rows(back[:, 2048:2560])
    in_tail_rows = in_tail.reshape(32, 8, 256)[:, :2].reshape(64, 256)
    token_part = dot(in_main.astype(bf16), back[:, :2048], ((0,), (0,))) + dot(
        in_tail_rows.astype(bf16), tail_rows, ((0,), (0,))
    )
    parts = back[:, 2560:2566].astype(f32)
    main_product = (parts[:, 0] + parts[:, 1] + parts[:, 2])[:, None]
    tail_product = (parts[:, 3] + parts[:, 4] + parts[:, 5]).reshape(32, 8)[:, :2].reshape(64, 1)
    of_token = jnp.sum(
        jnp.where(in_main, main_product, 0.0).reshape(32, 8, 256), axis=1
    ) + jnp.sum(jnp.where(in_tail_rows, tail_product, 0.0).reshape(32, 2, 256), axis=1)
    pair_product = jnp.stack(
        [jnp.sum(jnp.where(hit[k], of_token, 0.0), axis=0) for k in range(4)], axis=0
    )

    def block_for(dest):
        cols = lax.dynamic_slice_in_dim(token_part, 512 * dest, 512, 1)
        return cols

    token_sum = block_for(y)
    own_parts = in_parts(pair_product)
    product_sum = sum(v.astype(f32) for v in own_parts)
    flat = jnp.concatenate(own_parts + (jnp.zeros((4, 256), bf16),), axis=0)
    flat = jnp.concatenate([flat, jnp.zeros((16, 256), bf16)], axis=1)
    for shift in (1, 2, 3):
        dest = (y + shift) % 4
        message = jnp.concatenate([block_for(dest).astype(bf16), flat], axis=0)
        got = lax.ppermute(message, "tp", [(i, (i + shift) % 4) for i in range(4)])
        got = got.astype(f32)
        token_sum = token_sum + got[:256]
        product_sum = product_sum + got[256:260, :256] + got[260:264, :256] + got[264:268, :256]
    token_grad = token_sum.astype(bf16)
    gate_grad = (product_sum / weights_t).T
    return (token_grad, gate_grad, grads[0], grads[1], grads[2])


def solution(mesh):
    finer = Mesh(mesh.devices.reshape(8, 4, 2, mesh.shape["tp"]), ("ep_0", "ep_1", "ep_2", "tp"))
    in_specs = (
        P(EP, None),
        P(EP, None),
        P(EP, None),
        P(EP, None),
        P(EP, None, "tp"),
        P(EP, None, "tp"),
        P(EP, "tp", None),
    )
    out_specs = (P(EP, "tp"), P(EP, None), P(EP, None, "tp"), P(EP, None, "tp"), P(EP, "tp", None))
    return jax.shard_map(layer, mesh=finer, in_specs=in_specs, out_specs=out_specs, check_vma=False)
```

```python
import jax
import jax.numpy as jnp
from jax import lax
from jax.experimental import pallas as pl
from jax.experimental.pallas import tpu as pltpu
from jax.sharding import Mesh
from jax.sharding import PartitionSpec as P


EP = ("ep_0", "ep_1", "ep_2")
ZX = ("ep_0", "ep_1")
CY = ("ep_2", "tp")

clamp_limit = 7.0
sigmoid_slope = 1.702
bf16 = jnp.bfloat16
f32 = jnp.float32

SWAP = [(4, 3), (3, 4), (5, 2), (2, 5)]
PAIR_AWAY = [(4, 5), (5, 4), (2, 3), (3, 2)]
PAIR_HOME = [(0, 1), (1, 0), (6, 7), (7, 6)]
CORES = [(0, 1), (1, 0)]


def dot(a, b, dims, out=f32):
    return lax.dot_general(a, b, (dims, ((), ())), preferred_element_type=out)


def unit_backward(gate_pre, up_pre, hidden_grad):
    glu = jnp.minimum(gate_pre, clamp_limit)
    linear = jnp.clip(up_pre, -clamp_limit, clamp_limit)
    sigma = jax.nn.sigmoid(sigmoid_slope * glu)
    active = glu * sigma
    hidden = (active * (linear + 1.0)).astype(bf16)
    slope_term = sigma + sigmoid_slope * active * (1.0 - sigma)
    gate_pre_grad = jnp.where(
        gate_pre < clamp_limit, hidden_grad * (linear + 1.0) * slope_term, 0.0
    ).astype(bf16)
    up_pre_grad = jnp.where(jnp.abs(up_pre) < clamp_limit, hidden_grad * active, 0.0).astype(bf16)
    return hidden, gate_pre_grad, up_pre_grad


def in_parts(v):
    hi = lax.reduce_precision(v, 8, 7)
    mid = lax.reduce_precision(v - hi, 8, 7)
    low = lax.reduce_precision(v - hi - mid, 8, 7)
    return hi.astype(bf16), mid.astype(bf16), low.astype(bf16)


def call(body, out_shape, *operands, scratch=()):
    vmem = pl.BlockSpec(memory_space=pltpu.VMEM)
    return pl.pallas_call(
        body,
        out_shape=out_shape,
        in_specs=[vmem] * len(operands),
        out_specs=[vmem] * len(out_shape) if isinstance(out_shape, (list, tuple)) else vmem,
        compiler_params=pltpu.CompilerParams(vmem_limit_bytes=60 * 2**20),
    )(*operands)


def tail_pick(quarter):
    row = lax.broadcasted_iota(jnp.int32, (64, 256), 0)
    col = lax.broadcasted_iota(jnp.int32, (64, 256), 1)
    return (col == (row // 2) * 8 + quarter * 2 + row % 2).astype(f32).astype(bf16)


def tail_place(quarter):
    row = lax.broadcasted_iota(jnp.int32, (256, 64), 1)
    col = lax.broadcasted_iota(jnp.int32, (256, 64), 0)
    return (col == (row // 2) * 8 + quarter * 2 + row % 2).astype(f32).astype(bf16)


def expand(src, x, g, at):
    x[at : at + 256, :] = src[:, :2048]
    g[at : at + 256, :] = src[:, 2048:4096]
    for q in range(4):
        cols = slice(512 * q, 512 * q + 512)
        pick = tail_pick(q)
        x[at + 256 : at + 320, cols] = dot(pick, src[:, 4096:4608], ((1,), (0,))).astype(bf16)
        g[at + 256 : at + 320, cols] = dot(pick, src[:, 4608:5120], ((1,), (0,))).astype(bf16)


def units(x, g, acts, product, at, weights, copies):
    rows = slice(at, at + 320)
    total = jnp.zeros((320, 1), f32)
    for s, (wg, wu, wd) in enumerate(weights):
        for c in copies[3 * s : 3 * s + 3]:
            c.wait()
        gate_pre = dot(x[rows, :], wg[...], ((1,), (0,)))
        up_pre = dot(x[rows, :], wu[...], ((1,), (0,)))
        hidden_grad = dot(g[rows, :], wd[...], ((1,), (1,)))
        hidden, gg, ug = unit_backward(gate_pre, up_pre, hidden_grad)
        to = 768 * s
        acts[rows, to : to + 256] = hidden
        acts[rows, to + 256 : to + 512] = gg
        acts[rows, to + 512 : to + 768] = ug
        total = total + jnp.sum(hidden.astype(f32) * hidden_grad, axis=1, keepdims=True)
    product[...] = jnp.broadcast_to(total, (320, 128))


def row_sum(acts, at, cols, weights):
    total = jnp.zeros((320, 256), f32)
    for s, (wg, wu, _) in enumerate(weights):
        to = 768 * s
        gg = acts[at : at + 320, to + 256 : to + 512]
        ug = acts[at : at + 320, to + 512 : to + 768]
        total = total + dot(gg, wg[cols, :], ((1,), (1,))) + dot(ug, wu[cols, :], ((1,), (1,)))
    return total


def act_mine_body(
    mine, wg1, wu1, wd1, wg2, wu2, wd2, xm, gm, acts, product, own,
    src, x, g, vg1, vu1, vd1, vg2, vu2, vd2, sems,
):
    ins = ((mine, src), (wg1, vg1), (wu1, vu1), (wd1, vd1), (wg2, vg2), (wu2, vu2), (wd2, vd2))
    copies = [pltpu.make_async_copy(a, b, sems.at[i]) for i, (a, b) in enumerate(ins)]
    for c in copies:
        c.start()
    copies[0].wait()
    expand(src, x, g, 0)
    outs = [pltpu.make_async_copy(x, xm, sems.at[7]), pltpu.make_async_copy(g, gm, sems.at[8])]
    for c in outs:
        c.start()
    weights = ((vg1, vu1, vd1), (vg2, vu2, vd2))
    units(x, g, acts, product, 0, weights, copies[1:])

    def chunk(d, carry):
        cols = pl.ds(pl.multiple_of(d * 256, 256), 256)
        own[:, cols] = row_sum(acts, 0, cols, weights)
        return carry

    lax.fori_loop(0, 8, chunk, 0)
    for c in outs:
        c.wait()


def act_other_body(
    other, xm, gm, actm, wg1, wu1, wd1, wg2, wu2, wd2, xo, go, acts, hand_over, ag, au, ad,
    src, x, g, product, vg1, vu1, vd1, vg2, vu2, vd2, sems,
):
    first = pl.ds(0, 320)
    ins = (
        (other, src), (wg1, vg1), (wu1, vu1), (wd1, vd1), (wg2, vg2), (wu2, vu2), (wd2, vd2),
        (xm, x.at[first]), (gm, g.at[first]), (actm, acts.at[first]),
    )
    copies = [pltpu.make_async_copy(a, b, sems.at[i]) for i, (a, b) in enumerate(ins)]
    for c in copies:
        c.start()
    copies[0].wait()
    expand(src, x, g, 320)
    copies[7].wait()
    copies[8].wait()
    outs = [pltpu.make_async_copy(x, xo, sems.at[10]), pltpu.make_async_copy(g, go, sems.at[11])]
    for c in outs:
        c.start()
    weights = ((vg1, vu1, vd1), (vg2, vu2, vd2))
    units(x, g, acts, product, 320, weights, copies[1:7])
    copies[9].wait()

    def chunk(d, carry):
        cols = pl.ds(pl.multiple_of(d * 256, 256), 256)
        both = dot(x[:, cols], acts[:, 1024:1536], ((0,), (0,)))
        ag[cols, :] = both[:, :256].astype(bf16)
        au[cols, :] = both[:, 256:].astype(bf16)
        hand_over[:, cols] = row_sum(acts, 320, cols, weights).astype(bf16)
        return carry

    lax.fori_loop(0, 8, chunk, 0)
    ad[...] = dot(acts[:, 768:1024], g[...], ((0,), (0,))).astype(bf16)
    hi, mid, low = kernel_parts(product[...])
    lane = lax.broadcasted_iota(jnp.int32, (320, 128), 1)
    hand_over[:, 2048:] = jnp.where(
        lane == 0, hi.astype(f32), jnp.where(lane == 1, mid.astype(f32), low.astype(f32))
    ).astype(bf16)
    for c in outs:
        c.wait()


def weight_scratch():
    cols, rows = pltpu.VMEM((2048, 256), bf16), pltpu.VMEM((256, 2048), bf16)
    return [cols, cols, rows, cols, cols, rows]


def act_mine_call(*operands):
    shape = jax.ShapeDtypeStruct
    outs = [
        shape((320, 2048), bf16),
        shape((320, 2048), bf16),
        shape((320, 1536), bf16),
        shape((320, 128), f32),
        shape((320, 2048), f32),
    ]
    scratch = [pltpu.VMEM((256, 5120), bf16)] + [pltpu.VMEM((320, 2048), bf16)] * 2
    return copying_call(act_mine_body, outs, 2, operands, scratch + weight_scratch(), 9)


def act_other_call(*operands):
    shape = jax.ShapeDtypeStruct
    outs = [
        shape((640, 2048), bf16),
        shape((640, 2048), bf16),
        shape((640, 1536), bf16),
        shape((320, 2176), bf16),
        shape((2048, 256), bf16),
        shape((2048, 256), bf16),
        shape((256, 2048), bf16),
    ]
    scratch = [pltpu.VMEM((256, 5120), bf16)] + [pltpu.VMEM((640, 2048), bf16)] * 2
    scratch += [pltpu.VMEM((320, 128), f32)]
    return copying_call(act_other_body, outs, 2, operands, scratch + weight_scratch(), 12)


def copying_call(body, outs, copied, operands, scratch, count):
    vmem = pl.BlockSpec(memory_space=pltpu.VMEM)
    hbm = pl.BlockSpec(memory_space=pl.ANY)
    return pl.pallas_call(
        body,
        out_shape=outs,
        in_specs=[hbm] * len(operands),
        out_specs=[hbm] * copied + [vmem] * (len(outs) - copied),
        scratch_shapes=scratch + [pltpu.SemaphoreType.DMA((count,))],
        compiler_params=pltpu.CompilerParams(vmem_limit_bytes=60 * 2**20),
    )(*operands)


def prep_body(where, routes, weights, tokens, out_grad, send, key_out):
    kind, part = where[0], where[1]
    expert = 2 * lax.broadcasted_iota(jnp.int32, (32, 256), 0) + kind
    named = jnp.zeros((32, 256), f32)
    weight_of = jnp.zeros((32, 256), f32)
    for k in range(4):
        hit = routes[k : k + 1, :] == expert
        named = jnp.where(hit, 1.0, named)
        weight_of = jnp.where(hit, weights[k : k + 1, :], weight_of)
    before = lax.broadcasted_iota(jnp.int32, (256, 256), 0) < lax.broadcasted_iota(
        jnp.int32, (256, 256), 1
    )
    count = dot(named.astype(bf16), jnp.where(before, 1.0, 0.0).astype(bf16), ((1,), (0,)))
    rank = count.astype(jnp.int32) - 10 * part
    key = jnp.where((named > 0.0) & (rank >= 0) & (rank < 10), rank, -1)
    key_out[...] = key
    spread = jnp.broadcast_to(key[:, None, :], (32, 8, 256)).reshape(256, 256)
    spread_weight = jnp.broadcast_to(weight_of[:, None, :], (32, 8, 256)).reshape(256, 256)
    eighth = lax.broadcasted_iota(jnp.int32, (256, 256), 0) % 8
    quarter = lax.broadcasted_iota(jnp.int32, (256, 1), 0) % 8 // 2
    for n, wanted in enumerate((eighth, 8 + eighth % 2)):
        sel = jnp.where(spread == wanted, 1.0, 0.0)
        scale = jnp.sum(sel * spread_weight, axis=1, keepdims=True)
        pick = sel.astype(bf16)
        for m, src in enumerate((tokens, out_grad)):
            if n == 0:
                got = dot(pick, src[...], ((1,), (0,)))
            else:
                got = jnp.zeros((256, 512), f32)
                for q in range(4):
                    mine = jnp.where(quarter == q, sel, 0.0).astype(bf16)
                    got = got + dot(mine, src[:, 512 * q : 512 * q + 512], ((1,), (0,)))
            if m == 1:
                got = got * scale
            at = 4096 * n + got.shape[1] * m
            send[:, at : at + got.shape[1]] = got.astype(bf16)


def prep_call(*operands):
    vmem = pl.BlockSpec(memory_space=pltpu.VMEM)
    return pl.pallas_call(
        prep_body,
        out_shape=[
            jax.ShapeDtypeStruct((256, 5120), bf16),
            jax.ShapeDtypeStruct((32, 256), jnp.int32),
        ],
        in_specs=[pl.BlockSpec(memory_space=pltpu.SMEM)] + [vmem] * 4,
        out_specs=[vmem] * 2,
        compiler_params=pltpu.CompilerParams(vmem_limit_bytes=32 * 2**20),
    )(*operands)


def kernel_parts(v):
    hi = v.astype(bf16)
    mid = (v - hi.astype(f32)).astype(bf16)
    low = (v - hi.astype(f32) - mid.astype(f32)).astype(bf16)
    return hi, mid, low


def back_body(own, product, handed, back):
    back[:, :2048] = (own[:256, :] + handed[:256, :2048].astype(f32)).astype(bf16)
    tail = (own[256:320, :] + handed[256:320, :2048].astype(f32)).astype(bf16)
    lane = lax.broadcasted_iota(jnp.int32, (320, 128), 1)
    got = jnp.sum(
        jnp.where(lane < 3, handed[:, 2048:].astype(f32), 0.0), axis=1, keepdims=True
    )
    total = product[...] + got
    hi, mid, low = kernel_parts(total)
    spread = jnp.where(
        lane == 0, hi.astype(f32), jnp.where(lane == 1, mid.astype(f32), low.astype(f32))
    )
    placed = jnp.zeros((256, 512), f32)
    weights = jnp.zeros((256, 128), f32)
    for q in range(4):
        place = tail_place(q)
        placed = placed + dot(place, tail[:, 512 * q : 512 * q + 512], ((1,), (0,)))
        weights = weights + dot(place, spread[256:320].astype(bf16), ((1,), (0,)))
    back[:, 2048:2560] = placed.astype(bf16)
    back[:, 2560:2688] = jnp.where(lane[:256] < 3, spread[:256], 0.0).astype(bf16) + jnp.where(
        (lane[:256] >= 3) & (lane[:256] < 6), pltpu.roll(weights, 3, 1), 0.0
    ).astype(bf16)


def back_call(*operands):
    return call(back_body, jax.ShapeDtypeStruct((256, 2688), bf16), *operands)


def quarters_to_rows(tail):
    w = tail.shape[1]
    return tail.reshape(32, 4, 2, w).transpose(0, 2, 1, 3).reshape(64, 4 * w)


def layer(tokens, routes, gate_weights, out_grad, w_gate, w_up, w_down):
    y = lax.axis_index("tp")
    core = lax.axis_index("ep_2")
    kind = y // 2
    part = y % 2
    stays = core == kind

    home = (w_gate[0], w_up[0], w_down[0])
    came = [lax.ppermute(w, CY, SWAP + PAIR_HOME) for w in home]
    paired_away = [lax.ppermute(w, CY, PAIR_AWAY) for w in came]
    first = [jnp.where(stays, a, b) for a, b in zip(home, came)]
    first, came = lax.optimization_barrier((first, came))
    second = lax.optimization_barrier([jnp.where(stays, a, b) for a, b in zip(came, paired_away)])

    routes_t = routes.T
    weights_t = gate_weights.T
    send, key = prep_call(jnp.stack([kind, part]), routes_t, weights_t, tokens, out_grad)
    send = send.reshape(32, 8, 5120)
    expert = 2 * jnp.arange(32, dtype=jnp.int32)[:, None] + kind
    hit = [routes_t[k][None, :] == expert for k in range(4)]
    eight = jnp.arange(8, dtype=jnp.int32)[None, :, None]
    in_main = (key[:, None, :] == eight).reshape(256, 256)
    in_tail = (key[:, None, :] == 8 + eight % 2).reshape(256, 256)
    mine = lax.all_to_all(send, ZX, 0, 0, tiled=True)
    other = lax.ppermute(mine, "ep_2", CORES)
    xm, gm, actm, product, own_part = act_mine_call(mine.reshape(256, 5120), *first, *second)
    x, g, acts, hand_over, *away = act_other_call(
        other.reshape(256, 5120), xm, gm, actm, *first, *second
    )
    hidden, gg, ug = acts[:, :256], acts[:, 256:512], acts[:, 512:768]
    kept = (
        dot(x, gg, ((0,), (0,))),
        dot(x, ug, ((0,), (0,))),
        dot(hidden, g, ((0,), (0,))),
    )
    kept = lax.optimization_barrier(kept)
    got_away, came = [], []
    for i in range(3):
        got_away.append(lax.ppermute(away[i], CY, PAIR_AWAY))
        total = (kept[i] + got_away[i].astype(f32)).astype(bf16)
        came.append(lax.ppermute(jnp.where(stays, away[i], total), CY, SWAP + PAIR_HOME))
    grads = [
        (jnp.where(stays, a, 0.0) + b.astype(f32))[None] for a, b in zip(kept, came)
    ]

    handed = lax.ppermute(hand_over, "ep_2", CORES)
    back = back_call(own_part, product, handed).reshape(32, 8, 2688)
    back = lax.all_to_all(back, ZX, 0, 0, tiled=True).reshape(256, 2688)
    tail_rows = quarters_to_rows(back[:, 2048:2560])
    in_tail_rows = in_tail.reshape(32, 8, 256)[:, :2].reshape(64, 256)
    token_part = dot(in_main.astype(bf16), back[:, :2048], ((0,), (0,))) + dot(
        in_tail_rows.astype(bf16), tail_rows, ((0,), (0,))
    )
    parts = back[:, 2560:2566].astype(f32)
    main_product = (parts[:, 0] + parts[:, 1] + parts[:, 2])[:, None]
    tail_product = (parts[:, 3] + parts[:, 4] + parts[:, 5]).reshape(32, 8)[:, :2].reshape(64, 1)
    of_token = jnp.sum(
        jnp.where(in_main, main_product, 0.0).reshape(32, 8, 256), axis=1
    ) + jnp.sum(jnp.where(in_tail_rows, tail_product, 0.0).reshape(32, 2, 256), axis=1)
    pair_product = jnp.stack(
        [jnp.sum(jnp.where(hit[k], of_token, 0.0), axis=0) for k in range(4)], axis=0
    )

    def block_for(dest):
        cols = lax.dynamic_slice_in_dim(token_part, 512 * dest, 512, 1)
        return cols

    token_sum = block_for(y)
    own_parts = in_parts(pair_product)
    product_sum = sum(v.astype(f32) for v in own_parts)
    flat = jnp.concatenate(own_parts + (jnp.zeros((4, 256), bf16),), axis=0)
    flat = jnp.concatenate([flat, jnp.zeros((16, 256), bf16)], axis=1)
    for shift in (1, 2, 3):
        dest = (y + shift) % 4
        message = jnp.concatenate([block_for(dest).astype(bf16), flat], axis=0)
        got = lax.ppermute(message, "tp", [(i, (i + shift) % 4) for i in range(4)])
        got = got.astype(f32)
        token_sum = token_sum + got[:256]
        product_sum = product_sum + got[256:260, :256] + got[260:264, :256] + got[264:268, :256]
    token_grad = token_sum.astype(bf16)
    gate_grad = (product_sum / weights_t).T
    return (token_grad, gate_grad, grads[0], grads[1], grads[2])


def solution(mesh):
    finer = Mesh(mesh.devices.reshape(8, 4, 2, mesh.shape["tp"]), ("ep_0", "ep_1", "ep_2", "tp"))
    in_specs = (
        P(EP, None),
        P(EP, None),
        P(EP, None),
        P(EP, None),
        P(EP, None, "tp"),
        P(EP, None, "tp"),
        P(EP, "tp", None),
    )
    out_specs = (P(EP, "tp"), P(EP, None), P(EP, None, "tp"), P(EP, None, "tp"), P(EP, "tp", None))
    return jax.shard_map(layer, mesh=finer, in_specs=in_specs, out_specs=out_specs, check_vma=False)
```

```python
import jax
import jax.numpy as jnp
from jax import lax
from jax.experimental import pallas as pl
from jax.experimental.pallas import tpu as pltpu
from jax.sharding import Mesh
from jax.sharding import PartitionSpec as P


EP = ("ep_0", "ep_1", "ep_2")
ZX = ("ep_0", "ep_1")
CY = ("ep_2", "tp")

clamp_limit = 7.0
sigmoid_slope = 1.702
bf16 = jnp.bfloat16
f32 = jnp.float32

SWAP = [(4, 3), (3, 4), (5, 2), (2, 5)]
PAIR_AWAY = [(4, 5), (5, 4), (2, 3), (3, 2)]
PAIR_HOME = [(0, 1), (1, 0), (6, 7), (7, 6)]
CORES = [(0, 1), (1, 0)]


def dot(a, b, dims, out=f32):
    return lax.dot_general(a, b, (dims, ((), ())), preferred_element_type=out)


def unit_backward(gate_pre, up_pre, hidden_grad):
    glu = jnp.minimum(gate_pre, clamp_limit)
    linear = jnp.clip(up_pre, -clamp_limit, clamp_limit)
    sigma = jax.nn.sigmoid(sigmoid_slope * glu)
    active = glu * sigma
    hidden = (active * (linear + 1.0)).astype(bf16)
    slope_term = sigma + sigmoid_slope * active * (1.0 - sigma)
    gate_pre_grad = jnp.where(
        gate_pre < clamp_limit, hidden_grad * (linear + 1.0) * slope_term, 0.0
    ).astype(bf16)
    up_pre_grad = jnp.where(jnp.abs(up_pre) < clamp_limit, hidden_grad * active, 0.0).astype(bf16)
    return hidden, gate_pre_grad, up_pre_grad


def call(body, out_shape, *operands, scratch=()):
    vmem = pl.BlockSpec(memory_space=pltpu.VMEM)
    return pl.pallas_call(
        body,
        out_shape=out_shape,
        in_specs=[vmem] * len(operands),
        out_specs=[vmem] * len(out_shape) if isinstance(out_shape, (list, tuple)) else vmem,
        compiler_params=pltpu.CompilerParams(vmem_limit_bytes=60 * 2**20),
    )(*operands)


def tail_pick(quarter):
    row = lax.broadcasted_iota(jnp.int32, (64, 256), 0)
    col = lax.broadcasted_iota(jnp.int32, (64, 256), 1)
    return (col == (row // 2) * 8 + quarter * 2 + row % 2).astype(f32).astype(bf16)


def tail_place(quarter):
    row = lax.broadcasted_iota(jnp.int32, (256, 64), 1)
    col = lax.broadcasted_iota(jnp.int32, (256, 64), 0)
    return (col == (row // 2) * 8 + quarter * 2 + row % 2).astype(f32).astype(bf16)


def expand(src, x, g, at):
    x[at : at + 256, :] = src[:, :2048]
    g[at : at + 256, :] = src[:, 2048:4096]
    for q in range(4):
        cols = slice(512 * q, 512 * q + 512)
        pick = tail_pick(q)
        x[at + 256 : at + 320, cols] = dot(pick, src[:, 4096:4608], ((1,), (0,))).astype(bf16)
        g[at + 256 : at + 320, cols] = dot(pick, src[:, 4608:5120], ((1,), (0,))).astype(bf16)


def units(x, g, acts, product, at, weights, copies):
    rows = slice(at, at + 320)
    total = jnp.zeros((320, 1), f32)
    for s, (wg, wu, wd) in enumerate(weights):
        for c in copies[3 * s : 3 * s + 3]:
            c.wait()
        gate_pre = dot(x[rows, :], wg[...], ((1,), (0,)))
        up_pre = dot(x[rows, :], wu[...], ((1,), (0,)))
        hidden_grad = dot(g[rows, :], wd[...], ((1,), (1,)))
        hidden, gg, ug = unit_backward(gate_pre, up_pre, hidden_grad)
        to = 768 * s
        acts[rows, to : to + 256] = hidden
        acts[rows, to + 256 : to + 512] = gg
        acts[rows, to + 512 : to + 768] = ug
        total = total + jnp.sum(hidden.astype(f32) * hidden_grad, axis=1, keepdims=True)
    product[...] = jnp.broadcast_to(total, (320, 128))


def row_sum(acts, at, cols, weights):
    total = jnp.zeros((320, 256), f32)
    for s, (wg, wu, _) in enumerate(weights):
        to = 768 * s
        gg = acts[at : at + 320, to + 256 : to + 512]
        ug = acts[at : at + 320, to + 512 : to + 768]
        total = total + dot(gg, wg[cols, :], ((1,), (1,))) + dot(ug, wu[cols, :], ((1,), (1,)))
    return total


def act_mine_body(
    mine, wg1, wu1, wd1, wg2, wu2, wd2, xm, gm, acts, product, own,
    src, x, g, vg1, vu1, vd1, vg2, vu2, vd2, sems,
):
    ins = ((mine, src), (wg1, vg1), (wu1, vu1), (wd1, vd1), (wg2, vg2), (wu2, vu2), (wd2, vd2))
    copies = [pltpu.make_async_copy(a, b, sems.at[i]) for i, (a, b) in enumerate(ins)]
    for c in copies:
        c.start()
    copies[0].wait()
    expand(src, x, g, 0)
    outs = [pltpu.make_async_copy(x, xm, sems.at[7]), pltpu.make_async_copy(g, gm, sems.at[8])]
    for c in outs:
        c.start()
    weights = ((vg1, vu1, vd1), (vg2, vu2, vd2))
    units(x, g, acts, product, 0, weights, copies[1:])

    def chunk(d, carry):
        cols = pl.ds(pl.multiple_of(d * 256, 256), 256)
        own[:, cols] = row_sum(acts, 0, cols, weights)
        return carry

    lax.fori_loop(0, 8, chunk, 0)
    for c in outs:
        c.wait()


def act_other_body(
    other, xm, gm, actm, wg1, wu1, wd1, wg2, wu2, wd2, xo, go, acts, hand_over, ag, au, ad,
    src, x, g, product, vg1, vu1, vd1, vg2, vu2, vd2, sems,
):
    first = pl.ds(0, 320)
    ins = (
        (other, src), (wg1, vg1), (wu1, vu1), (wd1, vd1), (wg2, vg2), (wu2, vu2), (wd2, vd2),
        (xm, x.at[first]), (gm, g.at[first]), (actm, acts.at[first]),
    )
    copies = [pltpu.make_async_copy(a, b, sems.at[i]) for i, (a, b) in enumerate(ins)]
    for c in copies:
        c.start()
    copies[0].wait()
    expand(src, x, g, 320)
    copies[7].wait()
    copies[8].wait()
    outs = [pltpu.make_async_copy(x, xo, sems.at[10]), pltpu.make_async_copy(g, go, sems.at[11])]
    for c in outs:
        c.start()
    weights = ((vg1, vu1, vd1), (vg2, vu2, vd2))
    units(x, g, acts, product, 320, weights, copies[1:7])
    copies[9].wait()

    def chunk(d, carry):
        cols = pl.ds(pl.multiple_of(d * 256, 256), 256)
        both = dot(x[:, cols], acts[:, 1024:1536], ((0,), (0,)))
        ag[cols, :] = both[:, :256].astype(bf16)
        au[cols, :] = both[:, 256:].astype(bf16)
        hand_over[:, cols] = row_sum(acts, 320, cols, weights).astype(bf16)
        return carry

    lax.fori_loop(0, 8, chunk, 0)
    ad[...] = dot(acts[:, 768:1024], g[...], ((0,), (0,))).astype(bf16)
    hi, mid, low = kernel_parts(product[...])
    lane = lax.broadcasted_iota(jnp.int32, (320, 128), 1)
    hand_over[:, 2048:] = jnp.where(
        lane == 0, hi.astype(f32), jnp.where(lane == 1, mid.astype(f32), low.astype(f32))
    ).astype(bf16)
    for c in outs:
        c.wait()


def combine_body(where, key, routes, back, far, near, own):
    kind, y = where[0], where[1]
    spread = jnp.broadcast_to(key[...][:, None, :], (32, 8, 256)).reshape(256, 256)
    eighth = lax.broadcasted_iota(jnp.int32, (256, 256), 0) % 8
    main = jnp.where(spread == eighth, 1.0, 0.0)
    tail = jnp.where(spread == 8 + eighth % 2, 1.0, 0.0)
    main_t = main.T.astype(bf16)
    tail_t = tail.T
    quarter_t = lax.broadcasted_iota(jnp.int32, (256, 256), 1) % 8 // 2

    def block(dest):
        cols = pl.ds(pl.multiple_of(dest * 512, 512), 512)
        part = jnp.where(quarter_t == dest, tail_t, 0.0).astype(bf16)
        return dot(main_t, back[:, cols], ((1,), (0,))) + dot(
            part, back[:, 2048:2560], ((1,), (0,))
        )

    parts = back[:, 2560:2688].astype(f32)
    lane = lax.broadcasted_iota(jnp.int32, (256, 128), 1)
    main_product = jnp.sum(jnp.where(lane < 3, parts, 0.0), axis=1, keepdims=True)
    tail_product = jnp.sum(
        jnp.where((lane >= 3) & (lane < 6), parts, 0.0), axis=1, keepdims=True
    )
    placed = main * main_product + jnp.where(eighth < 2, tail, 0.0) * tail_product
    of_token = jnp.sum(placed.reshape(32, 8, 256), axis=1)
    expert = 2 * lax.broadcasted_iota(jnp.int32, (32, 256), 0) + kind
    row = lax.broadcasted_iota(jnp.int32, (16, 256), 0)
    flat = jnp.zeros((16, 256), f32)
    for k in range(4):
        hit = routes[k : k + 1, :] == expert
        pair = jnp.sum(jnp.where(hit, of_token, 0.0), axis=0, keepdims=True)
        for j, v in enumerate(kernel_parts(pair)):
            flat = jnp.where(row == 4 * j + k, v.astype(f32), flat)
    beside = y + 1 - 2 * (y % 2)
    across = 3 - y
    opposite = across + 1 - 2 * (across % 2)
    own[...] = block(y)
    near[:256, :] = block(beside)
    near[256:272, :256] = flat
    near[256:272, 256:] = jnp.zeros((16, 256), f32)
    far[:256, :512] = block(across).astype(bf16)
    far[:256, 512:] = block(opposite).astype(bf16)
    far[256:272, :512] = jnp.zeros((16, 512), bf16)
    far[256:272, 512:768] = flat.astype(bf16)
    far[256:272, 768:] = jnp.zeros((16, 256), bf16)


def combine_call(*operands):
    vmem = pl.BlockSpec(memory_space=pltpu.VMEM)
    shape = jax.ShapeDtypeStruct
    return pl.pallas_call(
        combine_body,
        out_shape=[
            shape((272, 1024), bf16),
            shape((272, 512), f32),
            shape((256, 512), f32),
        ],
        in_specs=[pl.BlockSpec(memory_space=pltpu.SMEM)] + [vmem] * 3,
        out_specs=[vmem] * 3,
        compiler_params=pltpu.CompilerParams(vmem_limit_bytes=32 * 2**20),
    )(*operands)


def weight_scratch():
    cols, rows = pltpu.VMEM((2048, 256), bf16), pltpu.VMEM((256, 2048), bf16)
    return [cols, cols, rows, cols, cols, rows]


def act_mine_call(*operands):
    shape = jax.ShapeDtypeStruct
    outs = [
        shape((320, 2048), bf16),
        shape((320, 2048), bf16),
        shape((320, 1536), bf16),
        shape((320, 128), f32),
        shape((320, 2048), f32),
    ]
    scratch = [pltpu.VMEM((256, 5120), bf16)] + [pltpu.VMEM((320, 2048), bf16)] * 2
    return copying_call(act_mine_body, outs, 2, operands, scratch + weight_scratch(), 9)


def act_other_call(*operands):
    shape = jax.ShapeDtypeStruct
    outs = [
        shape((640, 2048), bf16),
        shape((640, 2048), bf16),
        shape((640, 1536), bf16),
        shape((320, 2176), bf16),
        shape((2048, 256), bf16),
        shape((2048, 256), bf16),
        shape((256, 2048), bf16),
    ]
    scratch = [pltpu.VMEM((256, 5120), bf16)] + [pltpu.VMEM((640, 2048), bf16)] * 2
    scratch += [pltpu.VMEM((320, 128), f32)]
    return copying_call(act_other_body, outs, 2, operands, scratch + weight_scratch(), 12)


def copying_call(body, outs, copied, operands, scratch, count):
    vmem = pl.BlockSpec(memory_space=pltpu.VMEM)
    hbm = pl.BlockSpec(memory_space=pl.ANY)
    return pl.pallas_call(
        body,
        out_shape=outs,
        in_specs=[hbm] * len(operands),
        out_specs=[hbm] * copied + [vmem] * (len(outs) - copied),
        scratch_shapes=scratch + [pltpu.SemaphoreType.DMA((count,))],
        compiler_params=pltpu.CompilerParams(vmem_limit_bytes=60 * 2**20),
    )(*operands)


def prep_body(where, routes, weights, tokens, out_grad, send, key_out):
    kind, part = where[0], where[1]
    expert = 2 * lax.broadcasted_iota(jnp.int32, (32, 256), 0) + kind
    named = jnp.zeros((32, 256), f32)
    weight_of = jnp.zeros((32, 256), f32)
    for k in range(4):
        hit = routes[k : k + 1, :] == expert
        named = jnp.where(hit, 1.0, named)
        weight_of = jnp.where(hit, weights[k : k + 1, :], weight_of)
    before = lax.broadcasted_iota(jnp.int32, (256, 256), 0) < lax.broadcasted_iota(
        jnp.int32, (256, 256), 1
    )
    count = dot(named.astype(bf16), jnp.where(before, 1.0, 0.0).astype(bf16), ((1,), (0,)))
    rank = count.astype(jnp.int32) - 10 * part
    key = jnp.where((named > 0.0) & (rank >= 0) & (rank < 10), rank, -1)
    key_out[...] = key
    spread = jnp.broadcast_to(key[:, None, :], (32, 8, 256)).reshape(256, 256)
    spread_weight = jnp.broadcast_to(weight_of[:, None, :], (32, 8, 256)).reshape(256, 256)
    eighth = lax.broadcasted_iota(jnp.int32, (256, 256), 0) % 8
    quarter = lax.broadcasted_iota(jnp.int32, (256, 1), 0) % 8 // 2
    for n, wanted in enumerate((eighth, 8 + eighth % 2)):
        sel = jnp.where(spread == wanted, 1.0, 0.0)
        scale = jnp.sum(sel * spread_weight, axis=1, keepdims=True)
        pick = sel.astype(bf16)
        for m, src in enumerate((tokens, out_grad)):
            if n == 0:
                got = dot(pick, src[...], ((1,), (0,)))
            else:
                got = jnp.zeros((256, 512), f32)
                for q in range(4):
                    mine = jnp.where(quarter == q, sel, 0.0).astype(bf16)
                    got = got + dot(mine, src[:, 512 * q : 512 * q + 512], ((1,), (0,)))
            if m == 1:
                got = got * scale
            at = 4096 * n + got.shape[1] * m
            send[:, at : at + got.shape[1]] = got.astype(bf16)


def prep_call(*operands):
    vmem = pl.BlockSpec(memory_space=pltpu.VMEM)
    return pl.pallas_call(
        prep_body,
        out_shape=[
            jax.ShapeDtypeStruct((256, 5120), bf16),
            jax.ShapeDtypeStruct((32, 256), jnp.int32),
        ],
        in_specs=[pl.BlockSpec(memory_space=pltpu.SMEM)] + [vmem] * 4,
        out_specs=[vmem] * 2,
        compiler_params=pltpu.CompilerParams(vmem_limit_bytes=32 * 2**20),
    )(*operands)


def kernel_parts(v):
    hi = v.astype(bf16)
    mid = (v - hi.astype(f32)).astype(bf16)
    low = (v - hi.astype(f32) - mid.astype(f32)).astype(bf16)
    return hi, mid, low


def back_body(own, product, handed, back):
    back[:, :2048] = (own[:256, :] + handed[:256, :2048].astype(f32)).astype(bf16)
    tail = (own[256:320, :] + handed[256:320, :2048].astype(f32)).astype(bf16)
    lane = lax.broadcasted_iota(jnp.int32, (320, 128), 1)
    got = jnp.sum(
        jnp.where(lane < 3, handed[:, 2048:].astype(f32), 0.0), axis=1, keepdims=True
    )
    total = product[...] + got
    hi, mid, low = kernel_parts(total)
    spread = jnp.where(
        lane == 0, hi.astype(f32), jnp.where(lane == 1, mid.astype(f32), low.astype(f32))
    )
    placed = jnp.zeros((256, 512), f32)
    weights = jnp.zeros((256, 128), f32)
    for q in range(4):
        place = tail_place(q)
        placed = placed + dot(place, tail[:, 512 * q : 512 * q + 512], ((1,), (0,)))
        weights = weights + dot(place, spread[256:320].astype(bf16), ((1,), (0,)))
    back[:, 2048:2560] = placed.astype(bf16)
    back[:, 2560:2688] = jnp.where(lane[:256] < 3, spread[:256], 0.0).astype(bf16) + jnp.where(
        (lane[:256] >= 3) & (lane[:256] < 6), pltpu.roll(weights, 3, 1), 0.0
    ).astype(bf16)


def back_call(*operands):
    return call(back_body, jax.ShapeDtypeStruct((256, 2688), bf16), *operands)


def layer(tokens, routes, gate_weights, out_grad, w_gate, w_up, w_down):
    y = lax.axis_index("tp")
    core = lax.axis_index("ep_2")
    kind = y // 2
    part = y % 2
    stays = core == kind

    home = (w_gate[0], w_up[0], w_down[0])
    came = [lax.ppermute(w, CY, SWAP + PAIR_HOME) for w in home]
    paired_away = [lax.ppermute(w, CY, PAIR_AWAY) for w in came]
    first = [jnp.where(stays, a, b) for a, b in zip(home, came)]
    first, came = lax.optimization_barrier((first, came))
    second = lax.optimization_barrier([jnp.where(stays, a, b) for a, b in zip(came, paired_away)])

    routes_t = routes.T
    weights_t = gate_weights.T
    send, key = prep_call(jnp.stack([kind, part]), routes_t, weights_t, tokens, out_grad)
    send = send.reshape(32, 8, 5120)
    mine = lax.all_to_all(send, ZX, 0, 0, tiled=True)
    other = lax.ppermute(mine, "ep_2", CORES)
    xm, gm, actm, product, own_part = act_mine_call(mine.reshape(256, 5120), *first, *second)
    x, g, acts, hand_over, *away = act_other_call(
        other.reshape(256, 5120), xm, gm, actm, *first, *second
    )
    hidden, gg, ug = acts[:, :256], acts[:, 256:512], acts[:, 512:768]
    kept = (
        dot(x, gg, ((0,), (0,))),
        dot(x, ug, ((0,), (0,))),
        dot(hidden, g, ((0,), (0,))),
    )
    kept = lax.optimization_barrier(kept)
    got_away, came = [], []
    for i in range(3):
        got_away.append(lax.ppermute(away[i], CY, PAIR_AWAY))
        total = (kept[i] + got_away[i].astype(f32)).astype(bf16)
        came.append(lax.ppermute(jnp.where(stays, away[i], total), CY, SWAP + PAIR_HOME))
    grads = [
        (jnp.where(stays, a, 0.0) + b.astype(f32))[None] for a, b in zip(kept, came)
    ]

    handed = lax.ppermute(hand_over, "ep_2", CORES)
    back = back_call(own_part, product, handed).reshape(32, 8, 2688)
    back = lax.all_to_all(back, ZX, 0, 0, tiled=True).reshape(256, 2688)
    far, near, token_sum = combine_call(jnp.stack([kind, y]), key, routes_t, back)

    crossed = lax.ppermute(far, "tp", [(0, 3), (3, 0), (1, 2), (2, 1)])
    near = (near + crossed[:, 512:].astype(f32)).astype(bf16)
    paired = lax.ppermute(near, "tp", [(0, 1), (1, 0), (2, 3), (3, 2)])
    token_sum = token_sum + crossed[:256, :512].astype(f32) + paired[:256].astype(f32)
    flat = near[256:268, :256].astype(f32) + paired[256:268, :256].astype(f32)
    product_sum = flat[:4] + flat[4:8] + flat[8:]
    token_grad = token_sum.astype(bf16)
    gate_grad = (product_sum / weights_t).T
    return (token_grad, gate_grad, grads[0], grads[1], grads[2])


def solution(mesh):
    finer = Mesh(mesh.devices.reshape(8, 4, 2, mesh.shape["tp"]), ("ep_0", "ep_1", "ep_2", "tp"))
    in_specs = (
        P(EP, None),
        P(EP, None),
        P(EP, None),
        P(EP, None),
        P(EP, None, "tp"),
        P(EP, None, "tp"),
        P(EP, "tp", None),
    )
    out_specs = (P(EP, "tp"), P(EP, None), P(EP, None, "tp"), P(EP, None, "tp"), P(EP, "tp", None))
    return jax.shard_map(layer, mesh=finer, in_specs=in_specs, out_specs=out_specs, check_vma=False)
```

```python
import jax
import jax.numpy as jnp
from jax import lax
from jax.experimental import pallas as pl
from jax.experimental.pallas import tpu as pltpu
from jax.sharding import Mesh
from jax.sharding import PartitionSpec as P


EP = ("ep_0", "ep_1", "ep_2")
ZX = ("ep_0", "ep_1")
CY = ("ep_2", "tp")

clamp_limit = 7.0
sigmoid_slope = 1.702
bf16 = jnp.bfloat16
f32 = jnp.float32

SWAP = [(4, 3), (3, 4), (5, 2), (2, 5)]
PAIR_AWAY = [(4, 5), (5, 4), (2, 3), (3, 2)]
PAIR_HOME = [(0, 1), (1, 0), (6, 7), (7, 6)]
CORES = [(0, 1), (1, 0)]


def dot(a, b, dims, out=f32):
    return lax.dot_general(a, b, (dims, ((), ())), preferred_element_type=out)


def unit_backward(gate_pre, up_pre, hidden_grad):
    glu = jnp.minimum(gate_pre, clamp_limit)
    linear = jnp.clip(up_pre, -clamp_limit, clamp_limit)
    sigma = jax.nn.sigmoid(sigmoid_slope * glu)
    active = glu * sigma
    hidden = (active * (linear + 1.0)).astype(bf16)
    slope_term = sigma + sigmoid_slope * active * (1.0 - sigma)
    gate_pre_grad = jnp.where(
        gate_pre < clamp_limit, hidden_grad * (linear + 1.0) * slope_term, 0.0
    ).astype(bf16)
    up_pre_grad = jnp.where(jnp.abs(up_pre) < clamp_limit, hidden_grad * active, 0.0).astype(bf16)
    return hidden, gate_pre_grad, up_pre_grad


def call(body, out_shape, *operands, scratch=()):
    vmem = pl.BlockSpec(memory_space=pltpu.VMEM)
    return pl.pallas_call(
        body,
        out_shape=out_shape,
        in_specs=[vmem] * len(operands),
        out_specs=[vmem] * len(out_shape) if isinstance(out_shape, (list, tuple)) else vmem,
        compiler_params=pltpu.CompilerParams(vmem_limit_bytes=60 * 2**20),
    )(*operands)


def tail_pick(quarter):
    row = lax.broadcasted_iota(jnp.int32, (64, 256), 0)
    col = lax.broadcasted_iota(jnp.int32, (64, 256), 1)
    return (col == (row // 2) * 8 + quarter * 2 + row % 2).astype(f32).astype(bf16)


def tail_place(quarter):
    row = lax.broadcasted_iota(jnp.int32, (256, 64), 1)
    col = lax.broadcasted_iota(jnp.int32, (256, 64), 0)
    return (col == (row // 2) * 8 + quarter * 2 + row % 2).astype(f32).astype(bf16)


def expand(src, x, g, at):
    x[at : at + 256, :] = src[:, :2048]
    g[at : at + 256, :] = src[:, 2048:4096]
    for q in range(4):
        cols = slice(512 * q, 512 * q + 512)
        pick = tail_pick(q)
        x[at + 256 : at + 320, cols] = dot(pick, src[:, 4096:4608], ((1,), (0,))).astype(bf16)
        g[at + 256 : at + 320, cols] = dot(pick, src[:, 4608:5120], ((1,), (0,))).astype(bf16)


def units(x, g, acts, product, at, weights, copies):
    rows = slice(at, at + 320)
    total = jnp.zeros((320, 1), f32)
    for s, (wg, wu, wd) in enumerate(weights):
        for c in copies[3 * s : 3 * s + 3]:
            c.wait()
        gate_pre = dot(x[rows, :], wg[...], ((1,), (0,)))
        up_pre = dot(x[rows, :], wu[...], ((1,), (0,)))
        hidden_grad = dot(g[rows, :], wd[...], ((1,), (1,)))
        hidden, gg, ug = unit_backward(gate_pre, up_pre, hidden_grad)
        to = 768 * s
        acts[rows, to : to + 256] = hidden
        acts[rows, to + 256 : to + 512] = gg
        acts[rows, to + 512 : to + 768] = ug
        total = total + jnp.sum(hidden.astype(f32) * hidden_grad, axis=1, keepdims=True)
    product[...] = jnp.broadcast_to(total, (320, 128))


def row_sum(acts, at, cols, weights):
    total = jnp.zeros((320, 256), f32)
    for s, (wg, wu, _) in enumerate(weights):
        to = 768 * s
        gg = acts[at : at + 320, to + 256 : to + 512]
        ug = acts[at : at + 320, to + 512 : to + 768]
        total = total + dot(gg, wg[cols, :], ((1,), (1,))) + dot(ug, wu[cols, :], ((1,), (1,)))
    return total


def act_mine_body(
    mine, wg1, wu1, wd1, wg2, wu2, wd2, xm, gm, acts, product, own,
    src, x, g, vg1, vu1, vd1, vg2, vu2, vd2, sems,
):
    ins = ((mine, src), (wg1, vg1), (wu1, vu1), (wd1, vd1), (wg2, vg2), (wu2, vu2), (wd2, vd2))
    copies = [pltpu.make_async_copy(a, b, sems.at[i]) for i, (a, b) in enumerate(ins)]
    for c in copies:
        c.start()
    copies[0].wait()
    expand(src, x, g, 0)
    outs = [pltpu.make_async_copy(x, xm, sems.at[7]), pltpu.make_async_copy(g, gm, sems.at[8])]
    for c in outs:
        c.start()
    weights = ((vg1, vu1, vd1), (vg2, vu2, vd2))
    units(x, g, acts, product, 0, weights, copies[1:])

    def chunk(d, carry):
        cols = pl.ds(pl.multiple_of(d * 256, 256), 256)
        own[:, cols] = row_sum(acts, 0, cols, weights)
        return carry

    lax.fori_loop(0, 8, chunk, 0)
    for c in outs:
        c.wait()


def act_other_body(
    other, xm, gm, actm, wg1, wu1, wd1, wg2, wu2, wd2, xo, go, acts, hand_over, ag, au, ad,
    src, x, g, product, vg1, vu1, vd1, vg2, vu2, vd2, sems,
):
    first = pl.ds(0, 320)
    ins = (
        (other, src), (wg1, vg1), (wu1, vu1), (wd1, vd1), (wg2, vg2), (wu2, vu2), (wd2, vd2),
        (xm, x.at[first]), (gm, g.at[first]), (actm, acts.at[first]),
    )
    copies = [pltpu.make_async_copy(a, b, sems.at[i]) for i, (a, b) in enumerate(ins)]
    for c in copies:
        c.start()
    copies[0].wait()
    expand(src, x, g, 320)
    copies[7].wait()
    copies[8].wait()
    outs = [pltpu.make_async_copy(x, xo, sems.at[10]), pltpu.make_async_copy(g, go, sems.at[11])]
    for c in outs:
        c.start()
    weights = ((vg1, vu1, vd1), (vg2, vu2, vd2))
    units(x, g, acts, product, 320, weights, copies[1:7])
    copies[9].wait()

    def chunk(d, carry):
        cols = pl.ds(pl.multiple_of(d * 256, 256), 256)
        both = dot(x[:, cols], acts[:, 1024:1536], ((0,), (0,)))
        ag[cols, :] = both[:, :256].astype(bf16)
        au[cols, :] = both[:, 256:].astype(bf16)
        hand_over[:, cols] = row_sum(acts, 320, cols, weights).astype(bf16)
        return carry

    lax.fori_loop(0, 8, chunk, 0)
    ad[...] = dot(acts[:, 768:1024], g[...], ((0,), (0,))).astype(bf16)
    hi, mid, low = kernel_parts(product[...])
    lane = lax.broadcasted_iota(jnp.int32, (320, 128), 1)
    hand_over[:, 2048:] = jnp.where(
        lane == 0, hi.astype(f32), jnp.where(lane == 1, mid.astype(f32), low.astype(f32))
    ).astype(bf16)
    for c in outs:
        c.wait()


def combine_body(where, key, routes, back, m1, m2, m3, own):
    kind, y = where[0], where[1]
    spread = jnp.broadcast_to(key[...][:, None, :], (32, 8, 256)).reshape(256, 256)
    eighth = lax.broadcasted_iota(jnp.int32, (256, 256), 0) % 8
    main = jnp.where(spread == eighth, 1.0, 0.0)
    tail = jnp.where(spread == 8 + eighth % 2, 1.0, 0.0)
    main_t = main.T.astype(bf16)
    tail_t = tail.T
    quarter_t = lax.broadcasted_iota(jnp.int32, (256, 256), 1) % 8 // 2

    def block(shift):
        dest = (y + shift) % 4
        cols = pl.ds(pl.multiple_of(dest * 512, 512), 512)
        part = jnp.where(quarter_t == dest, tail_t, 0.0).astype(bf16)
        return dot(main_t, back[:, cols], ((1,), (0,))) + dot(
            part, back[:, 2048:2560], ((1,), (0,))
        )

    parts = back[:, 2560:2688].astype(f32)
    lane = lax.broadcasted_iota(jnp.int32, (256, 128), 1)
    main_product = jnp.sum(jnp.where(lane < 3, parts, 0.0), axis=1, keepdims=True)
    tail_product = jnp.sum(
        jnp.where((lane >= 3) & (lane < 6), parts, 0.0), axis=1, keepdims=True
    )
    placed = main * main_product + jnp.where(eighth < 2, tail, 0.0) * tail_product
    of_token = jnp.sum(placed.reshape(32, 8, 256), axis=1)
    expert = 2 * lax.broadcasted_iota(jnp.int32, (32, 256), 0) + kind
    row = lax.broadcasted_iota(jnp.int32, (16, 256), 0)
    flat = jnp.zeros((16, 256), f32)
    for k in range(4):
        hit = routes[k : k + 1, :] == expert
        pair = jnp.sum(jnp.where(hit, of_token, 0.0), axis=0, keepdims=True)
        for j, v in enumerate(kernel_parts(pair)):
            flat = jnp.where(row == 4 * j + k, v.astype(f32), flat)
    flat = flat.astype(bf16)
    zero = jnp.zeros((16, 256), bf16)
    own[...] = block(0)
    m1[:256, :] = block(1).astype(bf16)
    m2[:256, :] = block(2).astype(bf16)
    m3[:256, :] = block(3).astype(bf16)
    for m in (m1, m2, m3):
        m[256:272, :256] = flat
        m[256:272, 256:] = zero


def combine_call(*operands):
    vmem = pl.BlockSpec(memory_space=pltpu.VMEM)
    shape = jax.ShapeDtypeStruct
    return pl.pallas_call(
        combine_body,
        out_shape=[
            shape((272, 512), bf16),
            shape((272, 512), bf16),
            shape((272, 512), bf16),
            shape((256, 512), f32),
        ],
        in_specs=[pl.BlockSpec(memory_space=pltpu.SMEM)] + [vmem] * 3,
        out_specs=[vmem] * 4,
        compiler_params=pltpu.CompilerParams(vmem_limit_bytes=32 * 2**20),
    )(*operands)


def weight_scratch():
    cols, rows = pltpu.VMEM((2048, 256), bf16), pltpu.VMEM((256, 2048), bf16)
    return [cols, cols, rows, cols, cols, rows]


def act_mine_call(*operands):
    shape = jax.ShapeDtypeStruct
    outs = [
        shape((320, 2048), bf16),
        shape((320, 2048), bf16),
        shape((320, 1536), bf16),
        shape((320, 128), f32),
        shape((320, 2048), f32),
    ]
    scratch = [pltpu.VMEM((256, 5120), bf16)] + [pltpu.VMEM((320, 2048), bf16)] * 2
    return copying_call(act_mine_body, outs, 2, operands, scratch + weight_scratch(), 9)


def act_other_call(*operands):
    shape = jax.ShapeDtypeStruct
    outs = [
        shape((640, 2048), bf16),
        shape((640, 2048), bf16),
        shape((640, 1536), bf16),
        shape((320, 2176), bf16),
        shape((2048, 256), bf16),
        shape((2048, 256), bf16),
        shape((256, 2048), bf16),
    ]
    scratch = [pltpu.VMEM((256, 5120), bf16)] + [pltpu.VMEM((640, 2048), bf16)] * 2
    scratch += [pltpu.VMEM((320, 128), f32)]
    return copying_call(act_other_body, outs, 2, operands, scratch + weight_scratch(), 12)


def copying_call(body, outs, copied, operands, scratch, count):
    vmem = pl.BlockSpec(memory_space=pltpu.VMEM)
    hbm = pl.BlockSpec(memory_space=pl.ANY)
    return pl.pallas_call(
        body,
        out_shape=outs,
        in_specs=[hbm] * len(operands),
        out_specs=[hbm] * copied + [vmem] * (len(outs) - copied),
        scratch_shapes=scratch + [pltpu.SemaphoreType.DMA((count,))],
        compiler_params=pltpu.CompilerParams(vmem_limit_bytes=60 * 2**20),
    )(*operands)


def prep_body(where, routes, weights, tokens, out_grad, send, key_out):
    kind, part = where[0], where[1]
    expert = 2 * lax.broadcasted_iota(jnp.int32, (32, 256), 0) + kind
    named = jnp.zeros((32, 256), f32)
    weight_of = jnp.zeros((32, 256), f32)
    for k in range(4):
        hit = routes[k : k + 1, :] == expert
        named = jnp.where(hit, 1.0, named)
        weight_of = jnp.where(hit, weights[k : k + 1, :], weight_of)
    before = lax.broadcasted_iota(jnp.int32, (256, 256), 0) < lax.broadcasted_iota(
        jnp.int32, (256, 256), 1
    )
    count = dot(named.astype(bf16), jnp.where(before, 1.0, 0.0).astype(bf16), ((1,), (0,)))
    rank = count.astype(jnp.int32) - 10 * part
    key = jnp.where((named > 0.0) & (rank >= 0) & (rank < 10), rank, -1)
    key_out[...] = key
    spread = jnp.broadcast_to(key[:, None, :], (32, 8, 256)).reshape(256, 256)
    spread_weight = jnp.broadcast_to(weight_of[:, None, :], (32, 8, 256)).reshape(256, 256)
    eighth = lax.broadcasted_iota(jnp.int32, (256, 256), 0) % 8
    quarter = lax.broadcasted_iota(jnp.int32, (256, 1), 0) % 8 // 2
    for n, wanted in enumerate((eighth, 8 + eighth % 2)):
        sel = jnp.where(spread == wanted, 1.0, 0.0)
        scale = jnp.sum(sel * spread_weight, axis=1, keepdims=True)
        pick = sel.astype(bf16)
        for m, src in enumerate((tokens, out_grad)):
            if n == 0:
                got = dot(pick, src[...], ((1,), (0,)))
            else:
                got = jnp.zeros((256, 512), f32)
                for q in range(4):
                    mine = jnp.where(quarter == q, sel, 0.0).astype(bf16)
                    got = got + dot(mine, src[:, 512 * q : 512 * q + 512], ((1,), (0,)))
            if m == 1:
                got = got * scale
            at = 4096 * n + got.shape[1] * m
            send[:, at : at + got.shape[1]] = got.astype(bf16)


def prep_call(*operands):
    vmem = pl.BlockSpec(memory_space=pltpu.VMEM)
    return pl.pallas_call(
        prep_body,
        out_shape=[
            jax.ShapeDtypeStruct((256, 5120), bf16),
            jax.ShapeDtypeStruct((32, 256), jnp.int32),
        ],
        in_specs=[pl.BlockSpec(memory_space=pltpu.SMEM)] + [vmem] * 4,
        out_specs=[vmem] * 2,
        compiler_params=pltpu.CompilerParams(vmem_limit_bytes=32 * 2**20),
    )(*operands)


def kernel_parts(v):
    hi = v.astype(bf16)
    mid = (v - hi.astype(f32)).astype(bf16)
    low = (v - hi.astype(f32) - mid.astype(f32)).astype(bf16)
    return hi, mid, low


def back_body(own, product, handed, back):
    back[:, :2048] = (own[:256, :] + handed[:256, :2048].astype(f32)).astype(bf16)
    tail = (own[256:320, :] + handed[256:320, :2048].astype(f32)).astype(bf16)
    lane = lax.broadcasted_iota(jnp.int32, (320, 128), 1)
    got = jnp.sum(
        jnp.where(lane < 3, handed[:, 2048:].astype(f32), 0.0), axis=1, keepdims=True
    )
    total = product[...] + got
    hi, mid, low = kernel_parts(total)
    spread = jnp.where(
        lane == 0, hi.astype(f32), jnp.where(lane == 1, mid.astype(f32), low.astype(f32))
    )
    placed = jnp.zeros((256, 512), f32)
    weights = jnp.zeros((256, 128), f32)
    for q in range(4):
        place = tail_place(q)
        placed = placed + dot(place, tail[:, 512 * q : 512 * q + 512], ((1,), (0,)))
        weights = weights + dot(place, spread[256:320].astype(bf16), ((1,), (0,)))
    back[:, 2048:2560] = placed.astype(bf16)
    back[:, 2560:2688] = jnp.where(lane[:256] < 3, spread[:256], 0.0).astype(bf16) + jnp.where(
        (lane[:256] >= 3) & (lane[:256] < 6), pltpu.roll(weights, 3, 1), 0.0
    ).astype(bf16)


def back_call(*operands):
    return call(back_body, jax.ShapeDtypeStruct((256, 2688), bf16), *operands)


def layer(tokens, routes, gate_weights, out_grad, w_gate, w_up, w_down):
    y = lax.axis_index("tp")
    core = lax.axis_index("ep_2")
    kind = y // 2
    part = y % 2
    stays = core == kind

    home = (w_gate[0], w_up[0], w_down[0])
    came = [lax.ppermute(w, CY, SWAP + PAIR_HOME) for w in home]
    paired_away = [lax.ppermute(w, CY, PAIR_AWAY) for w in came]
    first = [jnp.where(stays, a, b) for a, b in zip(home, came)]
    first, came = lax.optimization_barrier((first, came))
    second = lax.optimization_barrier([jnp.where(stays, a, b) for a, b in zip(came, paired_away)])

    routes_t = routes.T
    weights_t = gate_weights.T
    send, key = prep_call(jnp.stack([kind, part]), routes_t, weights_t, tokens, out_grad)
    send = send.reshape(32, 8, 5120)
    mine = lax.all_to_all(send, ZX, 0, 0, tiled=True)
    other = lax.ppermute(mine, "ep_2", CORES)
    other = pltpu.with_memory_space_constraint(other.reshape(256, 5120), pltpu.VMEM)
    xm, gm, actm, product, own_part = act_mine_call(mine.reshape(256, 5120), *first, *second)
    x, g, acts, hand_over, *away = act_other_call(
        other, xm, gm, actm, *first, *second
    )
    hidden, gg, ug = acts[:, :256], acts[:, 256:512], acts[:, 512:768]
    kept = (
        dot(x, gg, ((0,), (0,))),
        dot(x, ug, ((0,), (0,))),
        dot(hidden, g, ((0,), (0,))),
    )
    kept = lax.optimization_barrier(kept)
    got_away, came = [], []
    for i in range(3):
        got_away.append(lax.ppermute(away[i], CY, PAIR_AWAY))
        total = (kept[i] + got_away[i].astype(f32)).astype(bf16)
        came.append(lax.ppermute(jnp.where(stays, away[i], total), CY, SWAP + PAIR_HOME))
    grads = [
        (jnp.where(stays, a, 0.0) + b.astype(f32))[None] for a, b in zip(kept, came)
    ]

    handed = lax.ppermute(hand_over, "ep_2", CORES)
    back = back_call(own_part, product, handed).reshape(32, 8, 2688)
    back = lax.all_to_all(back, ZX, 0, 0, tiled=True).reshape(256, 2688)
    *messages, token_sum = combine_call(jnp.stack([kind, y]), key, routes_t, back)

    flat = messages[0][256:268, :256].astype(f32)
    for shift in (2, 1, 3):
        got = lax.ppermute(
            messages[shift - 1], "tp", [(i, (i + shift) % 4) for i in range(4)]
        ).astype(f32)
        token_sum = token_sum + got[:256]
        flat = flat + got[256:268, :256]
    product_sum = flat[:4] + flat[4:8] + flat[8:]
    token_grad = token_sum.astype(bf16)
    gate_grad = (product_sum / weights_t).T
    return (token_grad, gate_grad, grads[0], grads[1], grads[2])


def solution(mesh):
    finer = Mesh(mesh.devices.reshape(8, 4, 2, mesh.shape["tp"]), ("ep_0", "ep_1", "ep_2", "tp"))
    in_specs = (
        P(EP, None),
        P(EP, None),
        P(EP, None),
        P(EP, None),
        P(EP, None, "tp"),
        P(EP, None, "tp"),
        P(EP, "tp", None),
    )
    out_specs = (P(EP, "tp"), P(EP, None), P(EP, None, "tp"), P(EP, None, "tp"), P(EP, "tp", None))
    return jax.shard_map(layer, mesh=finer, in_specs=in_specs, out_specs=out_specs, check_vma=False)
```
